1024 devices in a mesh: sp: 16 (over x, core), dp: 64 (over z, y).
Axes of the slice: x: 8, y: 8, z: 8, core: 2. Of those that a mesh axis runs over, the one named last changes fastest.
Arguments:
- cotangent: bfloat16 [64, 2048, 2048], P('dp', 'sp'), may hold values from -6 to 6
- layer_input: bfloat16 [64, 2048, 2048], P('dp', 'sp'), may hold values from -6 to 6
- x_pre: bfloat16 [64, 2048, 2048], P('dp', None, 'sp'), may hold values from -6 to 6
- z_pre: bfloat16 [64, 2048, 2048], P('dp', None, 'sp'), may hold values from -6 to 6
- b_pre: bfloat16 [64, 2048, 256], P('dp'), may hold values from -6 to 6
- c_pre: bfloat16 [64, 2048, 256], P('dp'), may hold values from -6 to 6
- dt_raw: bfloat16 [64, 2048, 32], P('dp', None, 'sp'), may hold values from -4.4 to 11.4
- conv_x: bfloat16 [4, 2048], P(None, 'sp'), may hold values from -3 to 3
- conv_b: bfloat16 [4, 256], replicated, may hold values from -3 to 3
- conv_c: bfloat16 [4, 256], replicated, may hold values from -3 to 3
- dt_bias: float32 [32], P('sp'), may hold values from -3.8 to -3.2
- a_log: float32 [32], P('sp'), may hold values from -9 to 0.5
- d_skip: float32 [32], P('sp'), may hold values from 0.5 to 1.5
- norm_w: float32 [2048], P('sp'), may hold values from 0.1 to 1.9
Outputs:
- d_x_pre: bfloat16 [64, 2048, 2048], P('dp', 'sp')
- d_z_pre: bfloat16 [64, 2048, 2048], P('dp', 'sp')
- d_b_pre: bfloat16 [64, 2048, 256], P('dp', 'sp')
- d_c_pre: bfloat16 [64, 2048, 256], P('dp', 'sp')
- d_dt_raw: bfloat16 [64, 2048, 32], P('dp', 'sp')
- grad_a_log: float32 [32], P('sp')
- grad_w_dt: float32 [2048, 32], replicated
The draws below stay inside these ranges and needn't reach their ends.
All inputs are finite; a program needn't handle non-finite values.
Results may differ from the reference program's by a relative error of at most 0.017.
Values may be sent and summed in bfloat16 or wider, within the bound.
A program may use at most 128 MiB of HBM per device.

```python
import jax
import jax.numpy as jnp
from jax import lax

D = 2048
HEADS = 32
HEAD_DIM = 64
GROUPS = 2
STATE = 128
CONV = 4
BLOCK = 128
TOK_DEV = 128
SEQ_LEN = 2048
NUM_STREAMS = 64
N_SP = 16


def draw_a_log(key, part):
    pick_key, spread_key = jax.random.split(jax.random.fold_in(key, 11))
    ranking = jax.random.permutation(pick_key, HEADS)
    gradual_decay_heads = ranking < HEADS // 2
    spread_draw = jax.random.uniform(spread_key, (HEADS,), jnp.float32)
    slow_rate = jnp.exp(jnp.log(0.3) + spread_draw * jnp.log(4.0)) / (TOK_DEV * N_SP)
    fast_rate = jnp.exp(jnp.log(1.0 / 60.0) + spread_draw * jnp.log(2.0))
    return jnp.log(jnp.where(gradual_decay_heads, slow_rate, fast_rate) / 0.03).astype(jnp.float32)


def draw_dt_raw(key, part):
    derived_prng_seeds = jax.random.split(jax.random.fold_in(key, 23), 3)
    overall_span_tokens = TOK_DEV * N_SP
    jitter = 0.6 * jnp.clip(jax.random.normal(derived_prng_seeds[0], (NUM_STREAMS, overall_span_tokens, HEADS), jnp.float32), -6.0, 6.0)
    block_level = jax.random.uniform(derived_prng_seeds[1], (NUM_STREAMS, N_SP, 1, HEADS), jnp.float32, minval=-0.7, maxval=0.7)
    offsets = jnp.broadcast_to(block_level, (NUM_STREAMS, N_SP, TOK_DEV, HEADS)).reshape(NUM_STREAMS, overall_span_tokens, HEADS)
    clustered_bundles = jax.random.randint(derived_prng_seeds[2], (NUM_STREAMS, 3), 0, overall_span_tokens)
    placement_indices = jnp.arange(overall_span_tokens)
    flagged_elements = jnp.any(placement_indices[None, :, None] == clustered_bundles[:, None, :], axis=2).astype(jnp.float32)
    return (jitter + offsets + 7.0 * flagged_elements[:, :, None]).astype(jnp.bfloat16)


def level_of(key, dims, cuts, low, largest):
    gain = 1.0
    for position, parts in cuts:
        steps = jax.random.uniform(jax.random.fold_in(jax.random.fold_in(key, 6), position), (parts,), jnp.float32, low / len(cuts), largest / len(cuts))
        gain = gain * jnp.repeat(jnp.exp(steps), dims[position] // parts).reshape((-1,) + (1,) * (len(dims) - 1 - position))
    return gain


def centred(stream_key, dims, width, reach, shards=(), held_as=jnp.bfloat16):
    level = level_of(stream_key, dims, shards, -0.22, 0.18) if shards else 1.0
    result = jax.random.normal(stream_key, dims, jnp.float32) * width * level
    return jnp.minimum(jnp.maximum(result, -reach), reach).astype(held_as)


def setup_inputs(seed: int = 0) -> dict:
    streams_of = jax.random.split(jax.random.key(seed), 15)
    return {
        "cotangent": centred(streams_of[0], (NUM_STREAMS, SEQ_LEN, HEADS * HEAD_DIM), 1.0, 6.0, ((0, 64), (1, 16))),
        "layer_input": centred(streams_of[1], (NUM_STREAMS, SEQ_LEN, D), 1.0, 6.0, ((0, 64), (1, 16))),
        "x_pre": centred(streams_of[2], (NUM_STREAMS, SEQ_LEN, HEADS * HEAD_DIM), 1.0, 6.0, ((0, 64), (2, 16))),
        "z_pre": centred(streams_of[3], (NUM_STREAMS, SEQ_LEN, HEADS * HEAD_DIM), 1.0, 6.0, ((0, 64), (2, 16))),
        "b_pre": centred(streams_of[4], (NUM_STREAMS, SEQ_LEN, GROUPS * STATE), 1.0, 6.0, ((0, 64),)),
        "c_pre": centred(streams_of[5], (NUM_STREAMS, SEQ_LEN, GROUPS * STATE), 1.0, 6.0, ((0, 64),)),
        "dt_raw": draw_dt_raw(jax.random.fold_in(streams_of[14], 71), 0),
        "conv_x": centred(streams_of[7], (CONV, HEADS * HEAD_DIM), CONV ** -0.5, 3.0, ((1, 16),)),
        "conv_b": centred(streams_of[8], (CONV, GROUPS * STATE), CONV ** -0.5, 3.0),
        "conv_c": centred(streams_of[9], (CONV, GROUPS * STATE), CONV ** -0.5, 3.0),
        "dt_bias": jnp.clip(-3.8 + 0.5999999 * jax.random.uniform(streams_of[10], (HEADS,), jnp.float32) ** level_of(streams_of[10], (HEADS,), ((0, 16),), -0.2, 0.2), -3.8, -3.2),
        "a_log": draw_a_log(jax.random.fold_in(streams_of[14], 71), 0),
        "d_skip": jnp.clip(0.5 + 1.0 * jax.random.uniform(streams_of[12], (HEADS,), jnp.float32) ** level_of(streams_of[12], (HEADS,), ((0, 16),), -0.2, 0.2), 0.5, 1.5),
        "norm_w": jnp.clip(1.0 + 0.18 * jax.random.normal(streams_of[13], (HEADS * HEAD_DIM,), jnp.float32), 0.1, 1.9),
    }


def causal_filter(signal, taps):
    tap_count = taps.shape[0]
    overall_span_tokens = signal.shape[1]
    padded = jnp.pad(signal, ((0, 0), (tap_count - 1, 0), (0, 0)))
    filtered = padded[:, 0:overall_span_tokens] * taps[0]
    for offset in range(1, tap_count):
        filtered = filtered + padded[:, offset:offset + overall_span_tokens] * taps[offset]
    return filtered

def mixer_out(x_input, state_source_vector, c_input, z_input, rate_raw, rate_log, x_filter, b_filter, readout_filter, rate_bias, skip_gain, norm_gain, block_len):
    highest = lax.Precision.HIGHEST
    seqs_here, overall_span_tokens, channels = x_input.shape
    head_count = rate_raw.shape[2]
    head_size = channels // head_count
    blocks = overall_span_tokens // block_len
    x_act = jax.nn.silu(causal_filter(x_input, x_filter))
    b_act = jax.nn.silu(causal_filter(state_source_vector, b_filter))
    c_act = jax.nn.silu(causal_filter(c_input, readout_filter))
    step_rate = jax.nn.softplus(rate_raw + rate_bias)
    log_step = -step_rate * jnp.exp(rate_log)
    x_heads = x_act.reshape(seqs_here, overall_span_tokens, head_count, head_size)
    scaled = (x_heads * step_rate[..., None]).reshape(seqs_here, blocks, block_len, head_count, head_size)
    b_blocks = b_act.reshape(seqs_here, blocks, block_len, -1)
    c_blocks = c_act.reshape(seqs_here, blocks, block_len, -1)
    cum_log = jnp.cumsum(jnp.swapaxes(log_step, 1, 2).reshape(seqs_here, head_count, blocks, block_len), axis=3)
    causal = jnp.tril(jnp.ones((block_len, block_len), dtype=bool))[None, None, None]
    spread = cum_log[..., :, None] - cum_log[..., None, :]
    decays = jnp.exp(jnp.where(causal, spread, -jnp.inf))
    scores = jnp.einsum('abln,absn->abls', c_blocks, b_blocks, precision=highest)
    within = jnp.einsum('arbls,absrp->ablrp', scores[:, None] * decays, scaled, precision=highest)
    to_end = jnp.transpose(jnp.exp(cum_log[..., -1:] - cum_log), (0, 2, 3, 1))
    pieces = jnp.einsum('absn,absrp->abrpn', b_blocks, scaled * to_end[..., None], precision=highest)
    block_fades = jnp.moveaxis(jnp.exp(cum_log[..., -1]), 2, 0)

    def carry_step(carried, inputs):
        addend, factor = inputs
        return (carried * factor[:, :, None, None] + addend, carried)
    initial = jnp.zeros((seqs_here, head_count, head_size, b_blocks.shape[-1]), jnp.float32)
    _, entering = lax.scan(carry_step, initial, (jnp.moveaxis(pieces, 1, 0), block_fades))
    entering = jnp.moveaxis(entering, 0, 1)
    from_start = jnp.transpose(jnp.exp(cum_log), (0, 2, 3, 1))
    carried_in = jnp.einsum('abln,abrpn->ablrp', c_blocks, entering, precision=highest) * from_start[..., None]
    mixed = (within + carried_in).reshape(seqs_here, overall_span_tokens, head_count, head_size) + skip_gain[:, None] * x_heads
    gated = mixed * jax.nn.silu(z_input.reshape(seqs_here, overall_span_tokens, head_count, head_size))
    inverse_rms = lax.rsqrt(lax.optimization_barrier(jnp.mean(gated * gated, axis=-1, keepdims=True)) + 1e-05)
    return (gated * inverse_rms * norm_gain.reshape(head_count, head_size)).reshape(seqs_here, overall_span_tokens, channels)

def reference(cotangent, layer_input, x_pre, z_pre, b_pre, c_pre, dt_raw, conv_x, conv_b, conv_c, dt_bias, a_log, d_skip, norm_w):
    runs = N_SP
    run_heads = HEADS // runs
    run_width = run_heads * HEAD_DIM
    group_span = runs // GROUPS
    overall_span_tokens = x_pre.shape[1]

    def by_run(values, each_width):
        return jnp.transpose(values.reshape(1, overall_span_tokens, runs, each_width), (2, 0, 1, 3))

    def by_group(values):
        repeated = jnp.repeat(values.reshape(1, overall_span_tokens, GROUPS, STATE), group_span, axis=2)
        return jnp.transpose(repeated, (2, 0, 1, 3))

    def back_tokens(values):
        return jnp.transpose(values, (1, 2, 0, 3)).reshape(overall_span_tokens, -1)
    x_taps = jnp.transpose(conv_x.astype(jnp.float32).reshape(CONV, runs, run_width), (1, 0, 2))
    b_taps = jnp.transpose(jnp.repeat(conv_b.astype(jnp.float32).reshape(CONV, GROUPS, STATE), group_span, axis=1), (1, 0, 2))
    c_taps = jnp.transpose(jnp.repeat(conv_c.astype(jnp.float32).reshape(CONV, GROUPS, STATE), group_span, axis=1), (1, 0, 2))
    bias_runs = dt_bias.reshape(runs, run_heads)
    log_runs = a_log.reshape(runs, run_heads)
    skip_runs = d_skip.reshape(runs, run_heads)
    gain_runs = norm_w.reshape(runs, run_width)

    def single_pass(x_in, b_in, c_in, z_in, rate_in, log_in, x_tap, b_tap, c_tap, bias_in, skip_in, gain_in, cot_in):

        def forward(x_input, state_source_vector, c_input, z_input, rate_raw, rate_log):
            return mixer_out(x_input, state_source_vector, c_input, z_input, rate_raw, rate_log, x_tap, b_tap, c_tap, bias_in, skip_in, gain_in, BLOCK)
        _, pullback = jax.vjp(forward, x_in, b_in, c_in, z_in, rate_in, log_in)
        return pullback(cot_in)

    def group_sum(partial_value):
        rounded = lax.optimization_barrier(partial_value.astype(jnp.bfloat16)).astype(jnp.float32)
        summed = lax.optimization_barrier(jnp.sum(rounded.reshape(GROUPS, group_span, overall_span_tokens, STATE), axis=1))
        return jnp.transpose(summed, (1, 0, 2)).reshape(overall_span_tokens, GROUPS * STATE).astype(jnp.bfloat16)

    def per_sequence(items):
        cot_seq, x_seq, z_seq, b_seq, c_seq, rate_seq = items
        gradients = jax.vmap(single_pass)(by_run(x_seq.astype(jnp.float32), run_width), by_group(b_seq.astype(jnp.float32)), by_group(c_seq.astype(jnp.float32)), by_run(z_seq.astype(jnp.float32), run_width), by_run(rate_seq.astype(jnp.float32), run_heads), log_runs, x_taps, b_taps, c_taps, bias_runs, skip_runs, gain_runs, by_run(cot_seq.astype(jnp.float32), run_width))
        grad_x, grad_b, grad_c, grad_z, grad_rate, grad_log = gradients
        return (back_tokens(grad_x).astype(jnp.bfloat16), back_tokens(grad_z).astype(jnp.bfloat16), group_sum(grad_b), group_sum(grad_c), back_tokens(grad_rate).astype(jnp.bfloat16), grad_log.reshape(HEADS))
    d_x_pre, d_z_pre, d_b_pre, d_c_pre, d_dt_raw, log_parts = lax.map(per_sequence, (cotangent, x_pre, z_pre, b_pre, c_pre, dt_raw))
    grad_a_log = lax.optimization_barrier(jnp.sum(log_parts, axis=0))
    grad_w_dt = jnp.dot(layer_input.reshape(-1, D).T, d_dt_raw.reshape(-1, HEADS), preferred_element_type=jnp.float32)
    return (d_x_pre, d_z_pre, d_b_pre, d_c_pre, d_dt_raw, grad_a_log, grad_w_dt)
```

```python
import functools
import math

import jax
import jax.numpy as jnp
from jax import lax
from jax.experimental import pallas as pl
from jax.experimental.pallas import tpu as pltpu
from jax.sharding import PartitionSpec as P

GROUPS = 2
STATE = 128
BLOCK = 128
TAPS = 4
HALF = 64
EPS = 1e-05
F32 = jnp.float32
BF16 = jnp.bfloat16


def mm(a, b, dims=((1,), (0,))):
    return lax.dot_general(a, b, (dims, ((), ())), preferred_element_type=F32)


def mm_exact(a, b):
    return lax.dot_general(
        a, b, (((1,), (0,)), ((), ())), precision=lax.Precision.HIGHEST, preferred_element_type=F32
    )


def split(v):
    high = v.astype(BF16)
    return high, (v - high.astype(F32)).astype(BF16)


def side(*parts):
    return jnp.concatenate(parts, axis=1)


def stack(*parts):
    return jnp.concatenate(parts, axis=0)


def mm3(a, b, ca, cb):
    join_a = side if ca else stack
    join_b = side if cb else stack
    dims = ((ca,), (cb,))
    return mm(join_a(*a), join_b(b[0], b[0]), dims) + mm(a[0], b[1], dims)


def pair_at(ref, at, start=0):
    return ref[at, start : start + 128], ref[at, start + 128 : start + 256]


def sigmoid(v):
    return 1.0 / (1.0 + jnp.exp(-v))


def taps_of(ref, start=None):
    whole = ref[...] if start is None else ref[:, pl.ds(start, 128)]
    whole = whole.astype(F32)
    return [whole[k : k + 1] for k in range(TAPS)]


def rows(j):
    return pl.ds(pl.multiple_of(j * BLOCK, BLOCK), BLOCK)


def kernel(
    n_sp,
    n_dp,
    cot_hbm,
    li_hbm,
    x_hbm,
    z_hbm,
    b_hbm,
    c_hbm,
    dt_ref,
    cx_ref,
    cb_ref,
    cc_ref,
    nw_ref,
    bias_ref,
    alog_ref,
    dskip_ref,
    dx_out,
    dz_out,
    db_out,
    dc_out,
    ddt_out,
    ga_out,
    gw_out,
    xv,
    zv,
    bv,
    cv,
    liv,
    cotv,
    dtrow,
    rowbuf,
    dcumbuf,
    rbuf,
    x_slope,
    b_act,
    b_slope,
    c_act,
    c_slope,
    decay0,
    decay1,
    scores,
    p_buf,
    xs_buf,
    y_buf,
    carried_buf,
    dy_buf,
    dt_e,
    cum_e,
    states,
    state,
    tails,
    dz_send,
    dx_send,
    bc_send,
    pair_rx,
    bc_sum,
    bc_rx,
    ddt_tx,
    ddt_rx,
    w_tx,
    w_rx,
    v_tx,
    v_rx,
    u_tx,
    u_rx,
    w_fin,
    loc,
    cot_s,
    cot_r,
    dz_s,
    dz_r,
    dx_s,
    dx_r,
    ddt_s,
    ddt_r,
    bc_s,
    bc_r,
    pair_s,
    pair_r,
    f_s,
    f_r,
    g_s,
    g_r,
    h_s,
    h_r,
    i_s,
    i_r,
    k_s,
    k_r,
):
    blocks = n_sp
    n_edge = math.isqrt(n_dp)
    chips = n_sp // 2
    w_tiles = w_fin.shape[0] // (n_edge * n_edge)
    me = lax.axis_index("sp")
    seq = lax.axis_index("dp")
    core = lax.rem(me, 2)
    chip = me // 2
    group = me // (n_sp // GROUPS)
    z_at = seq // n_edge
    y_at = lax.rem(seq, n_edge)
    first = y_at + core * (z_at - y_at)
    second = z_at + core * (y_at - z_at)
    group_at = pl.multiple_of(group * STATE, STATE)

    def wrap(i, n):
        return lax.rem(i + n, n)

    def along_first(k):
        return (z_at * n_edge + k) * (1 - core) + (k * n_edge + y_at) * core

    def along_second(k):
        return (k * n_edge + y_at) * (1 - core) + (z_at * n_edge + k) * core

    def to(src, dst, s_sem, r_sem, sp, dp):
        return pltpu.make_async_remote_copy(
            src_ref=src,
            dst_ref=dst,
            send_sem=s_sem,
            recv_sem=r_sem,
            device_id={"sp": sp, "dp": dp},
            device_id_type=pl.DeviceIdType.MESH,
        )

    def each(n, body):
        if n > 1:
            lax.fori_loop(1, n, lambda o, c: (body(o), c)[1], 0)

    loads = [
        pltpu.make_async_copy(x_hbm, xv, loc.at[0]),
        pltpu.make_async_copy(b_hbm.at[:, pl.ds(group_at, STATE)], bv, loc.at[1]),
        pltpu.make_async_copy(c_hbm.at[:, pl.ds(group_at, STATE)], cv, loc.at[2]),
        pltpu.make_async_copy(z_hbm, zv, loc.at[3]),
        pltpu.make_async_copy(li_hbm, liv, loc.at[4]),
        pltpu.make_async_copy(
            cot_hbm.at[:, pl.ds(pl.multiple_of(me * 128, 128), 128)], cotv.at[me], loc.at[5]
        ),
    ]
    for load in loads:
        load.start()

    barrier = pltpu.get_barrier_semaphore()

    def greet(sp, dp):
        pl.semaphore_signal(
            barrier, inc=1, device_id={"sp": sp, "dp": dp}, device_id_type=pl.DeviceIdType.MESH
        )

    each(n_sp, lambda o: greet(wrap(me + o, n_sp), seq))
    each(n_edge, lambda o: greet(me, along_first(wrap(first + o, n_edge))))
    each(n_edge, lambda o: greet(me, along_second(wrap(second + o, n_edge))))
    pl.semaphore_wait(barrier, (n_sp - 1) + 2 * (n_edge - 1))

    def cot_copy(peer, slot):
        return to(
            cot_hbm.at[:, pl.ds(pl.multiple_of(peer * 128, 128), 128)],
            cotv.at[slot],
            cot_s.at[peer],
            cot_r.at[slot],
            peer,
            seq,
        )

    each(n_sp, lambda o: cot_copy(wrap(me + o, n_sp), me).start())

    lane = lax.broadcasted_iota(jnp.int32, (BLOCK, 128), 1)
    row = lax.broadcasted_iota(jnp.int32, (BLOCK, 128), 0)
    low = lane < HALF
    causal = row >= lane
    lane1 = lax.broadcasted_iota(jnp.int32, (1, 128), 1)
    low1 = lane1 < HALF

    dtrow[...] = jnp.zeros_like(dtrow)
    for j in range(blocks):
        dtrow[j, 0:2, :] = dt_ref[:, j * BLOCK : (j + 1) * BLOCK].astype(F32)
    flat = (blocks * 8, 128)
    part = lax.rem(lax.broadcasted_iota(jnp.int32, flat, 0), 8)
    by_head = lambda ref: jnp.where(part == 0, ref[0], ref[1])
    raw = dtrow[...].reshape(flat) + by_head(bias_ref)
    rate = jnp.exp(by_head(alog_ref))
    dt = jnp.maximum(raw, 0.0) + jnp.log1p(jnp.exp(-jnp.abs(raw)))
    step = -dt * rate
    upto = (row <= lane).astype(F32)
    cum = mm_exact(step, upto)
    cum3 = cum.reshape(blocks, 8, 128)
    dt3 = dt.reshape(blocks, 8, 128)
    rowbuf[...] = jnp.where(
        lax.broadcasted_iota(jnp.int32, (blocks, 8, 128), 1) < 2, cum3, jnp.roll(dt3, 2, axis=1)
    )

    wx = taps_of(cx_ref)
    wb = taps_of(cb_ref, group_at)
    wc = taps_of(cc_ref, group_at)
    skip_e = jnp.where(low1, dskip_ref[0], dskip_ref[1])

    for i in range(4):
        loads[i].wait()

    tails[...] = jnp.zeros_like(tails)
    state[...] = jnp.zeros_like(state)

    def filtered(src, slot, taps, j):
        now = src[rows(j), :].astype(F32)
        window = jnp.concatenate([tails[slot], now], axis=0)
        tails[slot] = now[BLOCK - 8 :]
        total = now * taps[3]
        for k in range(3):
            total = total + window[5 + k : 5 + k + BLOCK] * taps[k]
        gate = sigmoid(total)
        act = total * gate
        return act, gate + act * (1.0 - gate)

    def halves(v):
        zero = jnp.zeros_like(v)
        return jnp.concatenate([jnp.where(low, v, zero), jnp.where(low, zero, v)], axis=0)

    def forward(j, carry):
        x_f, x_d = filtered(xv, 0, wx, j)
        b_f, b_d = filtered(bv, 1, wb, j)
        c_f, c_d = filtered(cv, 2, wc, j)
        at = rows(j)
        x_slope[at, :] = x_d
        b_p = split(b_f)
        c_p = split(c_f)
        b_act[at, :] = side(*b_p)
        b_slope[at, :] = b_d
        c_act[at, :] = side(*c_p)
        c_slope[at, :] = c_d
        own = rowbuf[j]
        columns = own.T
        cum_c0 = columns[:, 0:1]
        cum_c1 = columns[:, 1:2]
        dts = jnp.where(low, columns[:, 2:3], columns[:, 3:4])
        cums = jnp.where(low, cum_c0, cum_c1)
        dt_e[at, :] = dts
        cum_e[at, :] = cums
        l0 = jnp.where(causal, jnp.exp(jnp.minimum(cum_c0 - own[0:1], 0.0)), 0.0)
        l1 = jnp.where(causal, jnp.exp(jnp.minimum(cum_c1 - own[1:2], 0.0)), 0.0)
        decay0[at, :] = l0
        decay1[at, :] = l1
        sc = mm3(c_p, b_p, 1, 1)
        scores[at, :] = sc
        scaled = x_f * dts
        xs_hi, xs_lo = split(scaled)
        xs_buf[at, :] = side(xs_hi, xs_lo)
        last = cums[BLOCK - 1 : BLOCK]
        held = state[...]
        states[at, :] = held
        p0_hi, p0_lo = split(sc * l0)
        p1_hi, p1_lo = split(sc * l1)
        p_hi = side(p0_hi, p1_hi)
        p_lo = side(p0_lo, p1_lo)
        p_buf[at, :] = side(p_hi, p_lo)
        xs_h = halves(xs_hi)
        within = mm(p_hi, xs_h) + mm(p_lo, xs_h) + mm(p_hi, halves(xs_lo))
        brought = mm3(c_p, split(held), 1, 0) * jnp.exp(cums)
        carried_buf[at, :] = brought
        y_buf[at, :] = within + brought + skip_e * x_f
        ending = split(scaled * jnp.exp(last - cums))
        state[...] = held * jnp.exp(last) + mm3(b_p, ending, 0, 0)
        return carry

    lax.fori_loop(0, blocks, forward, 0)

    gain = nw_ref[...]
    segments = ((row < HALF) == low).astype(BF16)
    segments = jnp.concatenate([segments, segments], axis=0)

    def segment_mean(v):
        return mm(side(*split(v)), segments) * (1.0 / HALF)

    def gate_block(j):
        at = rows(j)
        y = y_buf[at, :]
        z = zv[at, :].astype(F32)
        gate = sigmoid(z)
        silz = z * gate
        gated = y * silz
        weighted = cotv[j].astype(F32) * gain
        inverse = lax.rsqrt(segment_mean(gated * gated) + EPS)
        mean2 = segment_mean(gated * weighted)
        d_gated = inverse * (weighted - gated * (inverse * inverse * mean2))
        dy_buf[at, :] = d_gated * silz
        dz_send[j] = (d_gated * y * (gate + silz * (1.0 - gate))).astype(BF16)

    def columns_of(ref, i):
        return ref.at[:, pl.ds(pl.multiple_of(i * 128, 128), 128)]

    def grad_copy(buf, out, s_sem, r_sem, peer, slot):
        return to(buf.at[peer], columns_of(out, slot), s_sem.at[peer], r_sem.at[slot], peer, seq)

    loads[5].wait()
    gate_block(me)
    dz_own = pltpu.make_async_copy(dz_send.at[me], columns_of(dz_out, me), loc.at[6])
    dz_own.start()

    def gate_next(o):
        j = wrap(me - o, n_sp)
        cot_copy(me, j).wait_recv()
        gate_block(j)
        grad_copy(dz_send, dz_out, dz_s, dz_r, j, me).start()

    each(n_sp, gate_next)

    tails[...] = jnp.zeros_like(tails)
    state[...] = jnp.zeros_like(state)

    def unfiltered(d, slot, taps):
        window = jnp.concatenate([d, tails[slot]], axis=0)
        tails[slot] = d[0:8]
        total = d * taps[3]
        for k in range(3):
            total = total + window[3 - k : 3 - k + BLOCK] * taps[k]
        return total

    def backward(i, carry):
        j = blocks - 1 - i
        at = rows(j)
        dy = dy_buf[at, :]
        dts = dt_e[at, :]
        cums = cum_e[at, :]
        b_p = pair_at(b_act, at)
        c_p = pair_at(c_act, at)
        l0 = decay0[at, :]
        l1 = decay1[at, :]
        sc = scores[at, :]
        xs_hi, xs_lo = pair_at(xs_buf, at)
        scaled = xs_hi.astype(F32) + xs_lo.astype(F32)
        last = cums[BLOCK - 1 : BLOCK]
        from_start = jnp.exp(cums)
        to_end = jnp.exp(last - cums)
        fade = jnp.exp(last)
        grad = state[...]
        grad_p = split(grad)
        held = states[at, :]
        dy_hi, dy_lo = split(dy)
        dy_hi = halves(dy_hi)
        dy_lo = halves(dy_lo)
        d_p = mm(side(dy_hi, dy_lo), side(xs_hi, xs_hi), ((1,), (1,))) + mm(
            dy_hi, xs_lo, ((1,), (1,))
        )
        d_p0 = d_p[:BLOCK]
        d_p1 = d_p[BLOCK:]
        d_sc = split(d_p0 * l0 + d_p1 * l1)
        m0 = d_p0 * (sc * l0)
        m1 = d_p1 * (sc * l1)
        p_hi = stack(*pair_at(p_buf, at))
        p_lo = stack(*pair_at(p_buf, at, 256))
        reached = mm3(b_p, grad_p, 1, 0)
        d_scaled = (
            mm(p_hi, dy_hi, ((0,), (0,)))
            + mm(p_lo, dy_hi, ((0,), (0,)))
            + mm(p_hi, dy_lo, ((0,), (0,)))
            + reached * to_end
        )
        start = split(dy * from_start)
        end_f = scaled * to_end
        d_x = d_scaled * dts + skip_e * dy
        dx_send[j] = unfiltered(d_x * x_slope[at, :], 0, wx).astype(BF16)
        d_c = mm3(d_sc, b_p, 1, 0) + mm3(start, split(held), 1, 1)
        d_b = mm3(d_sc, c_p, 0, 0) + mm3(split(end_f), grad_p, 1, 1)
        bc_send[j, :, 0:STATE] = unfiltered(d_b * b_slope[at, :], 1, wb).astype(BF16)
        bc_send[j, :, STATE:] = unfiltered(d_c * c_slope[at, :], 2, wc).astype(BF16)
        kept = reached * end_f
        diff = dy * carried_buf[at, :] - kept
        direct = d_scaled * scaled
        zero = jnp.zeros_like(diff)
        col0 = jnp.sum(m0 + jnp.where(low, diff, zero), axis=1, keepdims=True)
        col1 = jnp.sum(m1 + jnp.where(low, zero, diff), axis=1, keepdims=True)
        col2 = jnp.sum(jnp.where(low, direct, zero), axis=1, keepdims=True)
        col3 = jnp.sum(jnp.where(low, zero, direct), axis=1, keepdims=True)
        packed = jnp.where(
            lane == 0, col0, jnp.where(lane == 1, col1, jnp.where(lane == 2, col2, col3))
        )
        turned = packed.T[0:8]
        ends = jnp.sum(kept, axis=0, keepdims=True) + fade * jnp.sum(
            grad * held, axis=0, keepdims=True
        )
        end0 = jnp.sum(jnp.where(low1, ends, 0.0), axis=1, keepdims=True)
        end1 = jnp.sum(jnp.where(low1, 0.0, ends), axis=1, keepdims=True)
        at_end = lane1 == BLOCK - 1
        minus0 = jnp.where(at_end, end0, 0.0) - jnp.sum(m0, axis=0, keepdims=True)
        minus1 = jnp.where(at_end, end1, 0.0) - jnp.sum(m1, axis=0, keepdims=True)
        dcumbuf[j, 0:1, :] = turned[0:1] + minus0
        dcumbuf[j, 1:2, :] = turned[1:2] + minus1
        rbuf[j, 0:2, :] = turned[2:4]
        state[...] = grad * fade + mm3(c_p, start, 0, 0)
        return carry

    dcumbuf[...] = jnp.zeros_like(dcumbuf)
    rbuf[...] = jnp.zeros_like(rbuf)
    lax.fori_loop(0, blocks, backward, 0)

    since = (row >= lane).astype(F32)
    d_step = mm_exact(dcumbuf[...].reshape(flat), since)
    raw = dtrow[...].reshape(flat) + by_head(bias_ref)
    d_dt = rbuf[...].reshape(flat) / dt - d_step * rate
    d_raw = jnp.where(part < 2, d_dt * sigmoid(raw), 0.0)
    ddt_tx[...] = d_raw.astype(BF16).astype(F32).reshape(blocks, 8, 128)
    ga_part = jnp.sum((d_step * step).reshape(blocks, 8, 128), axis=0)

    def ddt_copy(peer, slot):
        return to(ddt_tx.at[peer], ddt_rx.at[slot], ddt_s.at[peer], ddt_r.at[slot], peer, seq)

    each(n_sp, lambda o: ddt_copy(wrap(me + o, n_sp), me).start())
    partner = me + 1 - 2 * core
    pair_copies = lambda q: to(
        bc_send.at[2 * q + 1 - core], pair_rx.at[q], pair_s.at[q], pair_r.at[q], partner, seq
    )
    lax.fori_loop(0, chips, lambda q, c: (pair_copies(q).start(), c)[1], 0)
    each(
        n_sp,
        lambda o: grad_copy(dx_send, dx_out, dx_s, dx_r, wrap(me + o, n_sp), me).start(),
    )
    dx_own = pltpu.make_async_copy(dx_send.at[me], columns_of(dx_out, me), loc.at[7])
    dx_own.start()
    ddt_rx[me] = ddt_tx[me]
    each(n_sp, lambda o: ddt_copy(me, wrap(me + o, n_sp)).wait_recv())

    heads = 2 * n_sp
    source = lax.broadcasted_iota(jnp.int32, (heads, blocks * 8), 1)
    target = lax.broadcasted_iota(jnp.int32, (heads, blocks * 8), 0)
    pick = (source == (target // 2) * 8 + lax.rem(target, 2)).astype(BF16)
    own_ddt = mm(pick, ddt_rx[...].reshape(flat).astype(BF16)).astype(BF16)
    ddt_out[...] = own_ddt
    loads[4].wait()
    per_row = liv.shape[1] // 128

    def place(t):
        y_of = (t // w_tiles) // n_edge
        z_of = (t // w_tiles) % n_edge
        a = y_of + core * (z_of - y_of)
        b = z_of + core * (y_of - z_of)
        return a, b, t % w_tiles

    for c0 in range(0, per_row, 4):
        piece = mm(own_ddt, liv[:, c0 * 128 : (c0 + 4) * 128])
        for r in range(heads // 8):
            for c in range(4):
                a, b, sub = place(r * per_row + c0 + c)
                w_tx[a, b * w_tiles + sub] = piece[8 * r : 8 * r + 8, c * 128 : (c + 1) * 128]
    lax.fori_loop(0, n_edge, lambda k, c: (w_tx.at[k].__setitem__(n_edge * w_tiles, ga_part), c)[1], 0)

    def first_copy(k, slot):
        return to(w_tx.at[k], w_rx.at[slot], f_s.at[k], f_r.at[slot], me, along_first(k))

    each(n_edge, lambda o: first_copy(wrap(first + o, n_edge), first).start())

    def pair_add(q, c):
        pair_copies(q).wait_recv()
        mine = bc_send[2 * q + core].astype(F32)
        bc_sum[q] = (mine + pair_rx[q].astype(F32)).astype(BF16)
        return c

    lax.fori_loop(0, chips, pair_add, 0)

    w_rx[first] = w_tx[first]
    each(n_edge, lambda o: first_copy(first, wrap(first + o, n_edge)).wait_recv())
    sum1 = w_rx[0]
    for k in range(1, n_edge):
        sum1 = sum1 + w_rx[k]
    for k in range(n_edge):
        v_tx[k, 0:w_tiles] = sum1[k * w_tiles : (k + 1) * w_tiles]
        v_tx[k, w_tiles] = sum1[n_edge * w_tiles]

    def second_copy(k, slot):
        return to(v_tx.at[k], v_rx.at[slot], g_s.at[k], g_r.at[slot], me, along_second(k))

    each(n_edge, lambda o: second_copy(wrap(second + o, n_edge), second).start())
    v_rx[second] = v_tx[second]
    each(n_edge, lambda o: second_copy(second, wrap(second + o, n_edge)).wait_recv())
    sum2 = v_rx[0]
    for k in range(1, n_edge):
        sum2 = sum2 + v_rx[k]
    ga_out[...] = jnp.broadcast_to(jnp.sum(sum2[w_tiles], axis=1, keepdims=True), (8, 128))
    u_tx[...] = sum2[0:w_tiles]

    def sp_copy(peer, slot):
        return to(u_tx, u_rx.at[slot], h_s.at[peer], h_r.at[slot], peer, seq)

    each(n_sp, lambda o: sp_copy(wrap(me + o, n_sp), me).start())

    def bc_copy(q, slot):
        return to(bc_sum.at[q], bc_rx.at[slot], bc_s.at[q], bc_r.at[slot], 2 * q + core, seq)

    each(chips, lambda o: bc_copy(wrap(chip + o, chips), chip).start())

    u_rx[me] = u_tx[...]
    each(n_sp, lambda o: sp_copy(me, wrap(me + o, n_sp)).wait_recv())
    sum3 = u_rx[0]
    for k in range(1, n_sp):
        sum3 = sum3 + u_rx[k]
    mine_at = (first * n_edge + second) * w_tiles
    w_fin[pl.ds(mine_at, w_tiles)] = sum3

    def gather2(k, slot):
        here = pl.ds((first * n_edge + slot) * w_tiles, w_tiles)
        return to(w_fin.at[here], w_fin.at[here], i_s.at[k], i_r.at[slot], me, along_second(k))

    each(n_edge, lambda o: gather2(wrap(second + o, n_edge), second).start())
    each(n_edge, lambda o: gather2(second, wrap(second + o, n_edge)).wait_recv())
    each(n_edge, lambda o: gather2(wrap(second + o, n_edge), second).wait_send())

    def gather1(k, slot):
        here = pl.ds(slot * n_edge * w_tiles, n_edge * w_tiles)
        return to(w_fin.at[here], w_fin.at[here], k_s.at[k], k_r.at[slot], me, along_first(k))

    each(n_edge, lambda o: gather1(wrap(first + o, n_edge), first).start())
    each(n_edge, lambda o: gather1(first, wrap(first + o, n_edge)).wait_recv())
    for t in range(w_fin.shape[0]):
        r, c = t // per_row, t % per_row
        a, b, sub = place(t)
        gw_out[8 * r : 8 * r + 8, c * 128 : (c + 1) * 128] = w_fin[
            (a * n_edge + b) * w_tiles + sub
        ]

    bc_rx[chip] = bc_sum[chip]
    each(chips, lambda o: bc_copy(chip, wrap(chip + o, chips)).wait_recv())
    span = chips // GROUPS
    for g in range(GROUPS):
        total = bc_rx[g * span].astype(F32)
        for q in range(1, span):
            total = total + bc_rx[g * span + q].astype(F32)
        db_out[:, g * STATE : (g + 1) * STATE] = total[:, 0:STATE].astype(BF16)
        dc_out[:, g * STATE : (g + 1) * STATE] = total[:, STATE:].astype(BF16)

    def finish(o):
        peer = wrap(me + o, n_sp)
        cot_copy(peer, me).wait_send()
        ddt_copy(peer, me).wait_send()
        sp_copy(peer, me).wait_send()
        dz = grad_copy(dz_send, dz_out, dz_s, dz_r, peer, me)
        dz.wait_send()
        grad_copy(dz_send, dz_out, dz_s, dz_r, me, peer).wait_recv()
        grad_copy(dx_send, dx_out, dx_s, dx_r, peer, me).wait_send()
        grad_copy(dx_send, dx_out, dx_s, dx_r, me, peer).wait_recv()

    each(n_sp, finish)
    lax.fori_loop(0, chips, lambda q, c: (pair_copies(q).wait_send(), c)[1], 0)
    each(chips, lambda o: bc_copy(wrap(chip + o, chips), chip).wait_send())

    def finish_edge(o):
        a = wrap(first + o, n_edge)
        b = wrap(second + o, n_edge)
        first_copy(a, first).wait_send()
        second_copy(b, second).wait_send()
        gather1(a, first).wait_send()

    each(n_edge, finish_edge)
    dz_own.wait()
    dx_own.wait()


def mixer(n_sp, n_dp, *args):
    n_edge = math.isqrt(n_dp)
    chips = n_sp // 2
    blocks = n_sp
    length = blocks * BLOCK
    width = n_sp * 128
    model = args[1].shape[1]
    heads = 2 * n_sp
    tiles = (heads // 8) * (model // 128)
    w_tiles = tiles // (n_edge * n_edge)
    any_space = pl.BlockSpec(memory_space=pl.ANY)
    vmem = pl.BlockSpec(memory_space=pltpu.VMEM)
    smem = pl.BlockSpec(memory_space=pltpu.SMEM)
    V = pltpu.VMEM
    seq_f = V((length, 128), F32)
    seq_b = V((length, 128), BF16)
    seq_d = V((length, 256), BF16)
    blk_b = V((blocks, BLOCK, 128), BF16)
    dma = lambda n: pltpu.SemaphoreType.DMA((n,))
    return pl.pallas_call(
        functools.partial(kernel, n_sp, n_dp),
        out_shape=(
            jax.ShapeDtypeStruct((BLOCK, width), BF16),
            jax.ShapeDtypeStruct((BLOCK, width), BF16),
            jax.ShapeDtypeStruct((BLOCK, GROUPS * STATE), BF16),
            jax.ShapeDtypeStruct((BLOCK, GROUPS * STATE), BF16),
            jax.ShapeDtypeStruct((heads, BLOCK), BF16),
            jax.ShapeDtypeStruct((8, 128), F32),
            jax.ShapeDtypeStruct((heads, model), F32),
        ),
        in_specs=[any_space] * 6 + [vmem] * 5 + [smem] * 3,
        out_specs=(any_space, any_space) + (vmem,) * 5,
        scratch_shapes=[
            seq_b,
            seq_b,
            seq_b,
            seq_b,
            V((BLOCK, model), BF16),
            blk_b,
            V((blocks, 8, 128), F32),
            V((blocks, 8, 128), F32),
            V((blocks, 8, 128), F32),
            V((blocks, 8, 128), F32),
            seq_f,
            seq_d,
            seq_f,
            seq_d,
            seq_f,
            seq_f,
            seq_f,
            seq_f,
            V((length, 4 * BLOCK), BF16),
            seq_d,
            seq_f,
            seq_f,
            seq_f,
            seq_f,
            seq_f,
            seq_f,
            V((STATE, 128), F32),
            V((3, 8, 128), F32),
            blk_b,
            blk_b,
            V((blocks, BLOCK, 2 * STATE), BF16),
            V((chips, BLOCK, 2 * STATE), BF16),
            V((chips, BLOCK, 2 * STATE), BF16),
            V((chips, BLOCK, 2 * STATE), BF16),
            V((blocks, 8, 128), F32),
            V((blocks, 8, 128), F32),
            V((n_edge, n_edge * w_tiles + 1, 8, 128), F32),
            V((n_edge, n_edge * w_tiles + 1, 8, 128), F32),
            V((n_edge, w_tiles + 1, 8, 128), F32),
            V((n_edge, w_tiles + 1, 8, 128), F32),
            V((w_tiles, 8, 128), F32),
            V((n_sp, w_tiles, 8, 128), F32),
            V((tiles, 8, 128), F32),
            dma(8),
            dma(n_sp),
            dma(n_sp),
            dma(n_sp),
            dma(n_sp),
            dma(n_sp),
            dma(n_sp),
            dma(n_sp),
            dma(n_sp),
            dma(chips),
            dma(chips),
            dma(chips),
            dma(chips),
            dma(n_edge),
            dma(n_edge),
            dma(n_edge),
            dma(n_edge),
            dma(n_sp),
            dma(n_sp),
            dma(n_edge),
            dma(n_edge),
            dma(n_edge),
            dma(n_edge),
        ],
        compiler_params=pltpu.CompilerParams(
            collective_id=0, has_side_effects=True, vmem_limit_bytes=60000 * 1024
        ),
        name="mixer_backward",
    )(*args)


def shards(
    n_sp,
    n_dp,
    cotangent,
    layer_input,
    x_pre,
    z_pre,
    b_pre,
    c_pre,
    dt_raw,
    conv_x,
    conv_b,
    conv_c,
    dt_bias,
    a_log,
    d_skip,
    norm_w,
):
    dx, dz, db, dc, ddt, ga, gw = mixer(
        n_sp,
        n_dp,
        cotangent[0],
        layer_input[0],
        x_pre[0],
        z_pre[0],
        b_pre[0],
        c_pre[0],
        dt_raw[0].T,
        conv_x,
        conv_b,
        conv_c,
        norm_w[None],
        dt_bias,
        a_log,
        d_skip,
    )
    return (dx[None], dz[None], db[None], dc[None], ddt.T[None], ga[0:2, 0], gw.T)


def solution(mesh):
    in_specs = (
        P("dp", "sp", None),
        P("dp", "sp", None),
        P("dp", None, "sp"),
        P("dp", None, "sp"),
        P("dp", None, None),
        P("dp", None, None),
        P("dp", None, "sp"),
        P(None, "sp"),
        P(),
        P(),
        P("sp"),
        P("sp"),
        P("sp"),
        P("sp"),
    )
    out_specs = (
        P("dp", "sp", None),
        P("dp", "sp", None),
        P("dp", "sp", None),
        P("dp", "sp", None),
        P("dp", "sp", None),
        P("sp"),
        P(),
    )
    return jax.shard_map(
        functools.partial(shards, mesh.shape["sp"], mesh.shape["dp"]),
        mesh=mesh,
        in_specs=in_specs,
        out_specs=out_specs,
        check_vma=False,
    )
```

```python
import functools

import jax
import jax.numpy as jnp
from jax import lax
from jax.experimental import pallas as pl
from jax.experimental.pallas import tpu as pltpu
from jax.sharding import PartitionSpec as P

GROUPS = 2
STATE = 128
BLOCK = 128
TAPS = 4
HALF = 64
EPS = 1e-05
F32 = jnp.float32
BF16 = jnp.bfloat16


def mm(a, b, dims=((1,), (0,))):
    return lax.dot_general(a, b, (dims, ((), ())), preferred_element_type=F32)


def mm_exact(a, b):
    return lax.dot_general(
        a, b, (((1,), (0,)), ((), ())), precision=lax.Precision.HIGHEST, preferred_element_type=F32
    )


def split(v):
    high = v.astype(BF16)
    return high, (v - high.astype(F32)).astype(BF16)


def side(*parts):
    return jnp.concatenate(parts, axis=1)


def stack(*parts):
    return jnp.concatenate(parts, axis=0)


def mm3(a, b, ca, cb):
    join_a = side if ca else stack
    join_b = side if cb else stack
    dims = ((ca,), (cb,))
    return mm(join_a(*a), join_b(b[0], b[0]), dims) + mm(a[0], b[1], dims)


def pair_at(ref, at, start=0):
    return ref[at, start : start + 128], ref[at, start + 128 : start + 256]


def sigmoid(v):
    return 1.0 / (1.0 + jnp.exp(-v))


def taps_of(ref, start=None):
    whole = ref[...] if start is None else ref[:, pl.ds(start, 128)]
    whole = whole.astype(F32)
    return [whole[k : k + 1] for k in range(TAPS)]


def rows(j):
    return pl.ds(pl.multiple_of(j * BLOCK, BLOCK), BLOCK)


def kernel(
    n_sp,
    n_dp,
    cot_hbm,
    li_hbm,
    x_hbm,
    z_hbm,
    b_hbm,
    c_hbm,
    dt_ref,
    cx_ref,
    cb_ref,
    cc_ref,
    nw_ref,
    bias_ref,
    alog_ref,
    dskip_ref,
    dx_out,
    dz_out,
    db_out,
    dc_out,
    ddt_out,
    ga_out,
    w_fin,
    xv,
    zv,
    bv,
    cv,
    liv,
    cotv,
    dtrow,
    rowbuf,
    dcumbuf,
    rbuf,
    x_slope,
    b_act,
    b_slope,
    c_act,
    c_slope,
    decay0,
    decay1,
    scores,
    p_buf,
    xs_buf,
    y_buf,
    carried_buf,
    dy_buf,
    dt_e,
    cum_e,
    states,
    state,
    tails,
    dz_send,
    dx_send,
    bc_send,
    pair_rx,
    bc_sum,
    bc_rx,
    ddt_tx,
    ddt_rx,
    w_tx,
    w_rx,
    u_tx,
    u_rx,
    loc,
    cot_s,
    cot_r,
    dz_s,
    dz_r,
    dx_s,
    dx_r,
    ddt_s,
    ddt_r,
    bc_s,
    bc_r,
    pair_s,
    pair_r,
    f_s,
    f_r,
    h_s,
    h_r,
    k_s,
    k_r,
):
    blocks = n_sp
    chips = n_sp // 2
    w_rows = w_fin.shape[1]
    w_tiles = w_rows // 8
    me = lax.axis_index("sp")
    seq = lax.axis_index("dp")
    core = lax.rem(me, 2)
    chip = me // 2
    group = me // (n_sp // GROUPS)
    group_at = pl.multiple_of(group * STATE, STATE)

    def wrap(i, n):
        return lax.rem(i + n, n)

    def to(src, dst, s_sem, r_sem, sp, dp):
        return pltpu.make_async_remote_copy(
            src_ref=src,
            dst_ref=dst,
            send_sem=s_sem,
            recv_sem=r_sem,
            device_id={"sp": sp, "dp": dp},
            device_id_type=pl.DeviceIdType.MESH,
        )

    def each(n, body):
        if n > 1:
            lax.fori_loop(1, n, lambda o, c: (body(o), c)[1], 0)

    loads = [
        pltpu.make_async_copy(x_hbm, xv, loc.at[0]),
        pltpu.make_async_copy(b_hbm.at[:, pl.ds(group_at, STATE)], bv, loc.at[1]),
        pltpu.make_async_copy(c_hbm.at[:, pl.ds(group_at, STATE)], cv, loc.at[2]),
        pltpu.make_async_copy(z_hbm, zv, loc.at[3]),
        pltpu.make_async_copy(li_hbm, liv, loc.at[4]),
        pltpu.make_async_copy(
            cot_hbm.at[:, pl.ds(pl.multiple_of(me * 128, 128), 128)], cotv.at[me], loc.at[5]
        ),
    ]
    for load in loads:
        load.start()

    barrier = pltpu.get_barrier_semaphore()

    def greet(sp, dp):
        pl.semaphore_signal(
            barrier, inc=1, device_id={"sp": sp, "dp": dp}, device_id_type=pl.DeviceIdType.MESH
        )

    each(n_sp, lambda o: greet(wrap(me + o, n_sp), seq))
    each(n_dp, lambda o: greet(me, wrap(seq + o, n_dp)))
    pl.semaphore_wait(barrier, (n_sp - 1) + (n_dp - 1))

    def cot_copy(peer, slot):
        return to(
            cot_hbm.at[:, pl.ds(pl.multiple_of(peer * 128, 128), 128)],
            cotv.at[slot],
            cot_s.at[peer],
            cot_r.at[slot],
            peer,
            seq,
        )

    each(n_sp, lambda o: cot_copy(wrap(me + o, n_sp), me).start())

    lane = lax.broadcasted_iota(jnp.int32, (BLOCK, 128), 1)
    row = lax.broadcasted_iota(jnp.int32, (BLOCK, 128), 0)
    low = lane < HALF
    causal = row >= lane
    lane1 = lax.broadcasted_iota(jnp.int32, (1, 128), 1)
    low1 = lane1 < HALF

    dtrow[...] = jnp.zeros_like(dtrow)
    for j in range(blocks):
        dtrow[j, 0:2, :] = dt_ref[:, j * BLOCK : (j + 1) * BLOCK].astype(F32)
    flat = (blocks * 8, 128)
    part = lax.rem(lax.broadcasted_iota(jnp.int32, flat, 0), 8)
    by_head = lambda ref: jnp.where(part == 0, ref[0], ref[1])
    raw = dtrow[...].reshape(flat) + by_head(bias_ref)
    rate = jnp.exp(by_head(alog_ref))
    dt = jnp.maximum(raw, 0.0) + jnp.log1p(jnp.exp(-jnp.abs(raw)))
    step = -dt * rate
    upto = (row <= lane).astype(F32)
    cum = mm_exact(step, upto)
    cum3 = cum.reshape(blocks, 8, 128)
    dt3 = dt.reshape(blocks, 8, 128)
    rowbuf[...] = jnp.where(
        lax.broadcasted_iota(jnp.int32, (blocks, 8, 128), 1) < 2, cum3, jnp.roll(dt3, 2, axis=1)
    )

    wx = taps_of(cx_ref)
    wb = taps_of(cb_ref, group_at)
    wc = taps_of(cc_ref, group_at)
    skip_e = jnp.where(low1, dskip_ref[0], dskip_ref[1])

    for i in range(4):
        loads[i].wait()

    tails[...] = jnp.zeros_like(tails)
    state[...] = jnp.zeros_like(state)

    def filtered(src, slot, taps, j):
        now = src[rows(j), :].astype(F32)
        window = jnp.concatenate([tails[slot], now], axis=0)
        tails[slot] = now[BLOCK - 8 :]
        total = now * taps[3]
        for k in range(3):
            total = total + window[5 + k : 5 + k + BLOCK] * taps[k]
        gate = sigmoid(total)
        act = total * gate
        return act, gate + act * (1.0 - gate)

    def halves(v):
        zero = jnp.zeros_like(v)
        return jnp.concatenate([jnp.where(low, v, zero), jnp.where(low, zero, v)], axis=0)

    def forward(j, carry):
        x_f, x_d = filtered(xv, 0, wx, j)
        b_f, b_d = filtered(bv, 1, wb, j)
        c_f, c_d = filtered(cv, 2, wc, j)
        at = rows(j)
        x_slope[at, :] = x_d
        b_p = split(b_f)
        c_p = split(c_f)
        b_act[at, :] = side(*b_p)
        b_slope[at, :] = b_d
        c_act[at, :] = side(*c_p)
        c_slope[at, :] = c_d
        own = rowbuf[j]
        columns = own.T
        cum_c0 = columns[:, 0:1]
        cum_c1 = columns[:, 1:2]
        dts = jnp.where(low, columns[:, 2:3], columns[:, 3:4])
        cums = jnp.where(low, cum_c0, cum_c1)
        dt_e[at, :] = dts
        cum_e[at, :] = cums
        l0 = jnp.where(causal, jnp.exp(jnp.minimum(cum_c0 - own[0:1], 0.0)), 0.0)
        l1 = jnp.where(causal, jnp.exp(jnp.minimum(cum_c1 - own[1:2], 0.0)), 0.0)
        decay0[at, :] = l0
        decay1[at, :] = l1
        sc = mm3(c_p, b_p, 1, 1)
        scores[at, :] = sc
        scaled = x_f * dts
        xs_hi, xs_lo = split(scaled)
        xs_buf[at, :] = side(xs_hi, xs_lo)
        last = cums[BLOCK - 1 : BLOCK]
        held = state[...]
        states[at, :] = held
        p0_hi, p0_lo = split(sc * l0)
        p1_hi, p1_lo = split(sc * l1)
        p_hi = side(p0_hi, p1_hi)
        p_lo = side(p0_lo, p1_lo)
        p_buf[at, :] = side(p_hi, p_lo)
        xs_h = halves(xs_hi)
        within = mm(p_hi, xs_h) + mm(p_lo, xs_h) + mm(p_hi, halves(xs_lo))
        brought = mm3(c_p, split(held), 1, 0) * jnp.exp(cums)
        carried_buf[at, :] = brought
        y_buf[at, :] = within + brought + skip_e * x_f
        ending = split(scaled * jnp.exp(last - cums))
        state[...] = held * jnp.exp(last) + mm3(b_p, ending, 0, 0)
        return carry

    lax.fori_loop(0, blocks, forward, 0)

    gain = nw_ref[...]
    segments = ((row < HALF) == low).astype(BF16)
    segments = jnp.concatenate([segments, segments], axis=0)

    def segment_mean(v):
        return mm(side(*split(v)), segments) * (1.0 / HALF)

    def gate_block(j):
        at = rows(j)
        y = y_buf[at, :]
        z = zv[at, :].astype(F32)
        gate = sigmoid(z)
        silz = z * gate
        gated = y * silz
        weighted = cotv[j].astype(F32) * gain
        inverse = lax.rsqrt(segment_mean(gated * gated) + EPS)
        mean2 = segment_mean(gated * weighted)
        d_gated = inverse * (weighted - gated * (inverse * inverse * mean2))
        dy_buf[at, :] = d_gated * silz
        dz_send[j] = (d_gated * y * (gate + silz * (1.0 - gate))).astype(BF16)

    def columns_of(ref, i):
        return ref.at[:, pl.ds(pl.multiple_of(i * 128, 128), 128)]

    def grad_copy(buf, out, s_sem, r_sem, peer, slot):
        return to(buf.at[peer], columns_of(out, slot), s_sem.at[peer], r_sem.at[slot], peer, seq)

    loads[5].wait()
    gate_block(me)
    dz_own = pltpu.make_async_copy(dz_send.at[me], columns_of(dz_out, me), loc.at[6])
    dz_own.start()

    def gate_next(o):
        j = wrap(me - o, n_sp)
        cot_copy(me, j).wait_recv()
        gate_block(j)
        grad_copy(dz_send, dz_out, dz_s, dz_r, j, me).start()

    each(n_sp, gate_next)

    tails[...] = jnp.zeros_like(tails)
    state[...] = jnp.zeros_like(state)

    def unfiltered(d, slot, taps):
        window = jnp.concatenate([d, tails[slot]], axis=0)
        tails[slot] = d[0:8]
        total = d * taps[3]
        for k in range(3):
            total = total + window[3 - k : 3 - k + BLOCK] * taps[k]
        return total

    def backward(i, carry):
        j = blocks - 1 - i
        at = rows(j)
        dy = dy_buf[at, :]
        dts = dt_e[at, :]
        cums = cum_e[at, :]
        b_p = pair_at(b_act, at)
        c_p = pair_at(c_act, at)
        l0 = decay0[at, :]
        l1 = decay1[at, :]
        sc = scores[at, :]
        xs_hi, xs_lo = pair_at(xs_buf, at)
        scaled = xs_hi.astype(F32) + xs_lo.astype(F32)
        last = cums[BLOCK - 1 : BLOCK]
        from_start = jnp.exp(cums)
        to_end = jnp.exp(last - cums)
        fade = jnp.exp(last)
        grad = state[...]
        grad_p = split(grad)
        held = states[at, :]
        dy_hi, dy_lo = split(dy)
        dy_hi = halves(dy_hi)
        dy_lo = halves(dy_lo)
        d_p = mm(side(dy_hi, dy_lo), side(xs_hi, xs_hi), ((1,), (1,))) + mm(
            dy_hi, xs_lo, ((1,), (1,))
        )
        d_p0 = d_p[:BLOCK]
        d_p1 = d_p[BLOCK:]
        d_sc = split(d_p0 * l0 + d_p1 * l1)
        m0 = d_p0 * (sc * l0)
        m1 = d_p1 * (sc * l1)
        p_hi = stack(*pair_at(p_buf, at))
        p_lo = stack(*pair_at(p_buf, at, 256))
        reached = mm3(b_p, grad_p, 1, 0)
        d_scaled = (
            mm(p_hi, dy_hi, ((0,), (0,)))
            + mm(p_lo, dy_hi, ((0,), (0,)))
            + mm(p_hi, dy_lo, ((0,), (0,)))
            + reached * to_end
        )
        start = split(dy * from_start)
        end_f = scaled * to_end
        d_x = d_scaled * dts + skip_e * dy
        dx_send[j] = unfiltered(d_x * x_slope[at, :], 0, wx).astype(BF16)
        d_c = mm3(d_sc, b_p, 1, 0) + mm3(start, split(held), 1, 1)
        d_b = mm3(d_sc, c_p, 0, 0) + mm3(split(end_f), grad_p, 1, 1)
        bc_send[j, :, 0:STATE] = unfiltered(d_b * b_slope[at, :], 1, wb).astype(BF16)
        bc_send[j, :, STATE:] = unfiltered(d_c * c_slope[at, :], 2, wc).astype(BF16)
        kept = reached * end_f
        diff = dy * carried_buf[at, :] - kept
        direct = d_scaled * scaled
        zero = jnp.zeros_like(diff)
        col0 = jnp.sum(m0 + jnp.where(low, diff, zero), axis=1, keepdims=True)
        col1 = jnp.sum(m1 + jnp.where(low, zero, diff), axis=1, keepdims=True)
        col2 = jnp.sum(jnp.where(low, direct, zero), axis=1, keepdims=True)
        col3 = jnp.sum(jnp.where(low, zero, direct), axis=1, keepdims=True)
        packed = jnp.where(
            lane == 0, col0, jnp.where(lane == 1, col1, jnp.where(lane == 2, col2, col3))
        )
        turned = packed.T[0:8]
        ends = jnp.sum(kept, axis=0, keepdims=True) + fade * jnp.sum(
            grad * held, axis=0, keepdims=True
        )
        end0 = jnp.sum(jnp.where(low1, ends, 0.0), axis=1, keepdims=True)
        end1 = jnp.sum(jnp.where(low1, 0.0, ends), axis=1, keepdims=True)
        at_end = lane1 == BLOCK - 1
        minus0 = jnp.where(at_end, end0, 0.0) - jnp.sum(m0, axis=0, keepdims=True)
        minus1 = jnp.where(at_end, end1, 0.0) - jnp.sum(m1, axis=0, keepdims=True)
        dcumbuf[j, 0:1, :] = turned[0:1] + minus0
        dcumbuf[j, 1:2, :] = turned[1:2] + minus1
        rbuf[j, 0:2, :] = turned[2:4]
        state[...] = grad * fade + mm3(c_p, start, 0, 0)
        return carry

    dcumbuf[...] = jnp.zeros_like(dcumbuf)
    rbuf[...] = jnp.zeros_like(rbuf)
    lax.fori_loop(0, blocks, backward, 0)

    since = (row >= lane).astype(F32)
    d_step = mm_exact(dcumbuf[...].reshape(flat), since)
    raw = dtrow[...].reshape(flat) + by_head(bias_ref)
    d_dt = rbuf[...].reshape(flat) / dt - d_step * rate
    d_raw = jnp.where(part < 2, d_dt * sigmoid(raw), 0.0)
    ddt_tx[...] = d_raw.astype(BF16).astype(F32).reshape(blocks, 8, 128)
    ga_part = jnp.sum((d_step * step).reshape(blocks, 8, 128), axis=0)

    def ddt_copy(peer, slot):
        return to(ddt_tx.at[peer], ddt_rx.at[slot], ddt_s.at[peer], ddt_r.at[slot], peer, seq)

    each(n_sp, lambda o: ddt_copy(wrap(me + o, n_sp), me).start())
    partner = me + 1 - 2 * core
    pair_copies = lambda q: to(
        bc_send.at[2 * q + 1 - core], pair_rx.at[q], pair_s.at[q], pair_r.at[q], partner, seq
    )
    lax.fori_loop(0, chips, lambda q, c: (pair_copies(q).start(), c)[1], 0)
    each(
        n_sp,
        lambda o: grad_copy(dx_send, dx_out, dx_s, dx_r, wrap(me + o, n_sp), me).start(),
    )
    dx_own = pltpu.make_async_copy(dx_send.at[me], columns_of(dx_out, me), loc.at[7])
    dx_own.start()
    ddt_rx[me] = ddt_tx[me]
    each(n_sp, lambda o: ddt_copy(me, wrap(me + o, n_sp)).wait_recv())

    heads = 2 * n_sp
    source = lax.broadcasted_iota(jnp.int32, (heads, blocks * 8), 1)
    target = lax.broadcasted_iota(jnp.int32, (heads, blocks * 8), 0)
    pick = (source == (target // 2) * 8 + lax.rem(target, 2)).astype(BF16)
    own_ddt = mm(pick, ddt_rx[...].reshape(flat).astype(BF16)).astype(BF16)
    ddt_out[...] = own_ddt
    loads[4].wait()
    per_row = liv.shape[1] // 128

    ga_sum = jnp.broadcast_to(jnp.sum(ga_part, axis=1, keepdims=True), (8, 128))
    ga_hi = ga_sum.astype(BF16).astype(F32)
    ga_row = jnp.where(low[0:8], ga_hi, ga_sum - ga_hi)
    for c0 in range(0, per_row, 4):
        piece = mm(own_ddt, liv[:, c0 * 128 : (c0 + 4) * 128])
        for r in range(heads // 8):
            for c in range(4):
                t = r * per_row + c0 + c
                tile = piece[8 * r : 8 * r + 8, c * 128 : (c + 1) * 128]
                if w_tiles == 1:
                    w_tx[t] = stack(tile, ga_row).astype(BF16)
                else:
                    at = (t % w_tiles) * 8
                    w_tx[t // w_tiles, at : at + 8, :] = tile.astype(BF16)
                    w_tx[t // w_tiles, w_rows:, :] = ga_row.astype(BF16)

    def scatter_copy(k, slot):
        return to(w_tx.at[k], w_rx.at[slot], f_s.at[k], f_r.at[slot], me, k)

    each(n_dp, lambda o: scatter_copy(wrap(seq + o, n_dp), seq).start())

    def pair_add(q, c):
        pair_copies(q).wait_recv()
        mine = bc_send[2 * q + core].astype(F32)
        bc_sum[q] = (mine + pair_rx[q].astype(F32)).astype(BF16)
        return c

    lax.fori_loop(0, chips, pair_add, 0)

    w_rx[seq] = w_tx[seq]
    each(n_dp, lambda o: scatter_copy(seq, wrap(seq + o, n_dp)).wait_recv())
    sum2 = lax.fori_loop(
        1, n_dp, lambda k, t: t + w_rx[k].astype(F32), w_rx[0].astype(F32), unroll=3 if n_dp == 64 else 1
    )
    ga_all = sum2[w_rows:]
    ga_out[...] = jnp.broadcast_to(ga_all[:, 0:1] + ga_all[:, HALF : HALF + 1], (8, 128))
    u_tx[...] = sum2[0:w_rows]

    def sp_copy(peer, slot):
        return to(u_tx, u_rx.at[slot], h_s.at[peer], h_r.at[slot], peer, seq)

    each(n_sp, lambda o: sp_copy(wrap(me + o, n_sp), me).start())

    def bc_copy(q, slot):
        return to(bc_sum.at[q], bc_rx.at[slot], bc_s.at[q], bc_r.at[slot], 2 * q + core, seq)

    each(chips, lambda o: bc_copy(wrap(chip + o, chips), chip).start())

    u_rx[me] = u_tx[...]
    each(n_sp, lambda o: sp_copy(me, wrap(me + o, n_sp)).wait_recv())
    sum3 = u_rx[0]
    for k in range(1, n_sp):
        sum3 = sum3 + u_rx[k]
    w_fin[seq] = sum3.astype(BF16)

    def gather_copy(k, slot):
        return to(w_fin.at[slot], w_fin.at[slot], k_s.at[k], k_r.at[slot], me, k)

    each(n_dp, lambda o: gather_copy(wrap(seq + o, n_dp), seq).start())

    bc_rx[chip] = bc_sum[chip]
    each(chips, lambda o: bc_copy(chip, wrap(chip + o, chips)).wait_recv())
    span = chips // GROUPS
    for g in range(GROUPS):
        total = bc_rx[g * span].astype(F32)
        for q in range(1, span):
            total = total + bc_rx[g * span + q].astype(F32)
        db_out[:, g * STATE : (g + 1) * STATE] = total[:, 0:STATE].astype(BF16)
        dc_out[:, g * STATE : (g + 1) * STATE] = total[:, STATE:].astype(BF16)

    def finish(o):
        peer = wrap(me + o, n_sp)
        cot_copy(peer, me).wait_send()
        ddt_copy(peer, me).wait_send()
        sp_copy(peer, me).wait_send()
        dz = grad_copy(dz_send, dz_out, dz_s, dz_r, peer, me)
        dz.wait_send()
        grad_copy(dz_send, dz_out, dz_s, dz_r, me, peer).wait_recv()
        grad_copy(dx_send, dx_out, dx_s, dx_r, peer, me).wait_send()
        grad_copy(dx_send, dx_out, dx_s, dx_r, me, peer).wait_recv()

    each(n_sp, finish)
    lax.fori_loop(0, chips, lambda q, c: (pair_copies(q).wait_send(), c)[1], 0)
    each(chips, lambda o: bc_copy(wrap(chip + o, chips), chip).wait_send())

    def finish_seq(o):
        peer = wrap(seq + o, n_dp)
        scatter_copy(peer, seq).wait_send()
        gather_copy(peer, seq).wait_send()
        gather_copy(seq, peer).wait_recv()

    each(n_dp, finish_seq)
    dz_own.wait()
    dx_own.wait()


def mixer(n_sp, n_dp, *args):
    chips = n_sp // 2
    blocks = n_sp
    length = blocks * BLOCK
    width = n_sp * 128
    model = args[1].shape[1]
    heads = 2 * n_sp
    tiles = (heads // 8) * (model // 128)
    w_rows = 8 * tiles // n_dp
    any_space = pl.BlockSpec(memory_space=pl.ANY)
    vmem = pl.BlockSpec(memory_space=pltpu.VMEM)
    smem = pl.BlockSpec(memory_space=pltpu.SMEM)
    V = pltpu.VMEM
    seq_f = V((length, 128), F32)
    seq_b = V((length, 128), BF16)
    seq_d = V((length, 256), BF16)
    blk_b = V((blocks, BLOCK, 128), BF16)
    dma = lambda n: pltpu.SemaphoreType.DMA((n,))
    parts = pl.pallas_call(
        functools.partial(kernel, n_sp, n_dp),
        out_shape=(
            jax.ShapeDtypeStruct((BLOCK, width), BF16),
            jax.ShapeDtypeStruct((BLOCK, width), BF16),
            jax.ShapeDtypeStruct((BLOCK, GROUPS * STATE), BF16),
            jax.ShapeDtypeStruct((BLOCK, GROUPS * STATE), BF16),
            jax.ShapeDtypeStruct((heads, BLOCK), BF16),
            jax.ShapeDtypeStruct((8, 128), F32),
            jax.ShapeDtypeStruct((n_dp, w_rows, 128), BF16),
        ),
        in_specs=[any_space] * 6 + [vmem] * 5 + [smem] * 3,
        out_specs=(any_space, any_space) + (vmem,) * 5,
        scratch_shapes=[
            seq_b,
            seq_b,
            seq_b,
            seq_b,
            V((BLOCK, model), BF16),
            blk_b,
            V((blocks, 8, 128), F32),
            V((blocks, 8, 128), F32),
            V((blocks, 8, 128), F32),
            V((blocks, 8, 128), F32),
            seq_f,
            seq_d,
            seq_f,
            seq_d,
            seq_f,
            seq_f,
            seq_f,
            seq_f,
            V((length, 4 * BLOCK), BF16),
            seq_d,
            seq_f,
            seq_f,
            seq_f,
            seq_f,
            seq_f,
            seq_f,
            V((STATE, 128), F32),
            V((3, 8, 128), F32),
            blk_b,
            blk_b,
            V((blocks, BLOCK, 2 * STATE), BF16),
            V((chips, BLOCK, 2 * STATE), BF16),
            V((chips, BLOCK, 2 * STATE), BF16),
            V((chips, BLOCK, 2 * STATE), BF16),
            V((blocks, 8, 128), F32),
            V((blocks, 8, 128), F32),
            V((n_dp, w_rows + 8, 128), BF16),
            V((n_dp, w_rows + 8, 128), BF16),
            V((w_rows, 128), F32),
            V((n_sp, w_rows, 128), F32),
            dma(8),
            dma(n_sp),
            dma(n_sp),
            dma(n_sp),
            dma(n_sp),
            dma(n_sp),
            dma(n_sp),
            dma(n_sp),
            dma(n_sp),
            dma(chips),
            dma(chips),
            dma(chips),
            dma(chips),
            dma(n_dp),
            dma(n_dp),
            dma(n_sp),
            dma(n_sp),
            dma(n_dp),
            dma(n_dp),
        ],
        compiler_params=pltpu.CompilerParams(
            collective_id=0, has_side_effects=True, vmem_limit_bytes=60000 * 1024
        ),
        name="mixer_backward",
    )(*args)
    return pl.pallas_call(
        finish_kernel,
        out_shape=tuple(jax.ShapeDtypeStruct(p.shape, p.dtype) for p in parts[:5])
        + (jax.ShapeDtypeStruct((2,), F32), jax.ShapeDtypeStruct((heads, model), F32)),
        in_specs=[vmem] * 7,
        out_specs=(vmem,) * 5 + (smem, vmem),
        name="finish",
    )(*parts)


def finish_kernel(dx, dz, db, dc, ddt, ga, w, dx_out, dz_out, db_out, dc_out, ddt_out, ga_out, gw_out):
    dx_out[...] = dx[...]
    dz_out[...] = dz[...]
    db_out[...] = db[...]
    dc_out[...] = dc[...]
    ddt_out[...] = ddt[...]
    ga_out[0] = ga[0, 0]
    ga_out[1] = ga[1, 0]
    per_row = gw_out.shape[1] // 128
    w_tiles = w.shape[1] // 8
    for t in range(w.shape[0] * w_tiles):
        r, c, at = t // per_row, t % per_row, 8 * (t % w_tiles)
        gw_out[8 * r : 8 * r + 8, c * 128 : (c + 1) * 128] = w[t // w_tiles, at : at + 8, :].astype(F32)


def shards(
    n_sp,
    n_dp,
    cotangent,
    layer_input,
    x_pre,
    z_pre,
    b_pre,
    c_pre,
    dt_raw,
    conv_x,
    conv_b,
    conv_c,
    dt_bias,
    a_log,
    d_skip,
    norm_w,
):
    dx, dz, db, dc, ddt, ga, gw = mixer(
        n_sp,
        n_dp,
        cotangent[0],
        layer_input[0],
        x_pre[0],
        z_pre[0],
        b_pre[0],
        c_pre[0],
        dt_raw[0].T,
        conv_x,
        conv_b,
        conv_c,
        norm_w[None],
        dt_bias,
        a_log,
        d_skip,
    )
    return (dx[None], dz[None], db[None], dc[None], ddt.T[None], ga, gw.T)


def solution(mesh):
    in_specs = (
        P("dp", "sp", None),
        P("dp", "sp", None),
        P("dp", None, "sp"),
        P("dp", None, "sp"),
        P("dp", None, None),
        P("dp", None, None),
        P("dp", None, "sp"),
        P(None, "sp"),
        P(),
        P(),
        P("sp"),
        P("sp"),
        P("sp"),
        P("sp"),
    )
    out_specs = (
        P("dp", "sp", None),
        P("dp", "sp", None),
        P("dp", "sp", None),
        P("dp", "sp", None),
        P("dp", "sp", None),
        P("sp"),
        P(),
    )
    return jax.shard_map(
        functools.partial(shards, mesh.shape["sp"], mesh.shape["dp"]),
        mesh=mesh,
        in_specs=in_specs,
        out_specs=out_specs,
        check_vma=False,
    )
```

```python
import functools
import math

import jax
import jax.numpy as jnp
from jax import lax
from jax.experimental import pallas as pl
from jax.experimental.pallas import tpu as pltpu
from jax.sharding import PartitionSpec as P

GROUPS = 2
STATE = 128
BLOCK = 128
TAPS = 4
HALF = 64
EPS = 1e-05
DZ_EARLY = 6
DX_EARLY = 15
F32 = jnp.float32
BF16 = jnp.bfloat16


def mm(a, b, dims=((1,), (0,))):
    return lax.dot_general(a, b, (dims, ((), ())), preferred_element_type=F32)


def mm_exact(a, b):
    return lax.dot_general(
        a, b, (((1,), (0,)), ((), ())), precision=lax.Precision.HIGHEST, preferred_element_type=F32
    )


def split(v):
    high = v.astype(BF16)
    return high, (v - high.astype(F32)).astype(BF16)


def side(*parts):
    return jnp.concatenate(parts, axis=1)


def stack(*parts):
    return jnp.concatenate(parts, axis=0)


def mm3(a, b, ca, cb):
    join_a = side if ca else stack
    join_b = side if cb else stack
    dims = ((ca,), (cb,))
    return mm(join_a(*a), join_b(b[0], b[0]), dims) + mm(a[0], b[1], dims)


def pair_at(ref, at, start=0):
    return ref[at, start : start + 128], ref[at, start + 128 : start + 256]


def sigmoid(v):
    return 1.0 / (1.0 + jnp.exp(-v))


def taps_of(ref, start=None):
    whole = ref[...] if start is None else ref[:, pl.ds(start, 128)]
    whole = whole.astype(F32)
    return [whole[k : k + 1] for k in range(TAPS)]


def rows(j):
    return pl.ds(pl.multiple_of(j * BLOCK, BLOCK), BLOCK)


def kernel(
    n_sp,
    n_dp,
    cot_hbm,
    li_hbm,
    x_hbm,
    z_hbm,
    b_hbm,
    c_hbm,
    dt_ref,
    cx_ref,
    cb_ref,
    cc_ref,
    nw_ref,
    bias_ref,
    alog_ref,
    dskip_ref,
    dx_out,
    dz_out,
    db_out,
    dc_out,
    ddt_out,
    ga_out,
    w_fin,
    xv,
    zv,
    bv,
    cv,
    liv,
    cotv,
    dtrow,
    rowbuf,
    dcumbuf,
    rbuf,
    x_slope,
    b_act,
    b_slope,
    c_act,
    c_slope,
    decay0,
    decay1,
    scores,
    p_buf,
    xs_buf,
    y_buf,
    carried_buf,
    dy_buf,
    dt_e,
    cum_e,
    states,
    state,
    tails,
    dz_send,
    dx_send,
    bc_send,
    pair_rx,
    bc_sum,
    bc_rx,
    ddt_tx,
    ddt_rx,
    w_tx,
    w_rx,
    u_tx,
    u_rx,
    ga_tx,
    ga_rx,
    loc,
    cot_s,
    cot_r,
    dz_s,
    dz_r,
    dx_s,
    dx_r,
    ddt_s,
    ddt_r,
    bc_s,
    bc_r,
    pair_s,
    pair_r,
    f_s,
    f_r,
    h_s,
    h_r,
    k_s,
    k_r,
    ga_s,
    ga_r,
):
    blocks = n_sp
    chips = n_sp // 2
    w_rows = w_fin.shape[1]
    w_tiles = w_rows // 8
    me = lax.axis_index("sp")
    seq = lax.axis_index("dp")
    core = lax.rem(me, 2)
    chip = me // 2
    group = me // (n_sp // GROUPS)
    group_at = pl.multiple_of(group * STATE, STATE)

    def wrap(i, n):
        return lax.rem(i + n, n)

    def hop(p, n):
        odd = p % 2 if isinstance(p, int) else lax.rem(p, 2)
        return ((p + 1) // 2) * odd + (n - p // 2) * (1 - odd)

    def ahead(p):
        return wrap(me + hop(p, n_sp), n_sp)

    def behind(p):
        return wrap(me - hop(p, n_sp), n_sp)

    def to(src, dst, s_sem, r_sem, sp, dp):
        return pltpu.make_async_remote_copy(
            src_ref=src,
            dst_ref=dst,
            send_sem=s_sem,
            recv_sem=r_sem,
            device_id={"sp": sp, "dp": dp},
            device_id_type=pl.DeviceIdType.MESH,
        )

    def each(n, body):
        if n > 1:
            lax.fori_loop(1, n, lambda o, c: (body(o), c)[1], 0)

    def some(low_o, high_o, body):
        lax.fori_loop(low_o, high_o, lambda o, c: (body(o), c)[1], 0)

    loads = [
        pltpu.make_async_copy(x_hbm, xv, loc.at[0]),
        pltpu.make_async_copy(b_hbm.at[:, pl.ds(group_at, STATE)], bv, loc.at[1]),
        pltpu.make_async_copy(c_hbm.at[:, pl.ds(group_at, STATE)], cv, loc.at[2]),
        pltpu.make_async_copy(z_hbm, zv, loc.at[3]),
        pltpu.make_async_copy(li_hbm, liv, loc.at[4]),
        pltpu.make_async_copy(
            cot_hbm.at[:, pl.ds(pl.multiple_of(me * 128, 128), 128)], cotv.at[me], loc.at[5]
        ),
    ]
    for load in loads:
        load.start()

    barrier = pltpu.get_barrier_semaphore()

    def greet(sp, dp):
        pl.semaphore_signal(
            barrier, inc=1, device_id={"sp": sp, "dp": dp}, device_id_type=pl.DeviceIdType.MESH
        )

    each(n_sp, lambda o: greet(wrap(me + o, n_sp), seq))
    each(n_dp, lambda o: greet(me, wrap(seq + o, n_dp)))
    def cot_copy(peer, slot):
        return to(
            cot_hbm.at[:, pl.ds(pl.multiple_of(peer * 128, 128), 128)],
            cotv.at[slot],
            cot_s.at[peer],
            cot_r.at[slot],
            peer,
            seq,
        )

    pl.semaphore_wait(barrier, (n_sp - 1) + (n_dp - 1))
    each(n_sp, lambda o: cot_copy(ahead(o), me).start())

    lane = lax.broadcasted_iota(jnp.int32, (BLOCK, 128), 1)
    row = lax.broadcasted_iota(jnp.int32, (BLOCK, 128), 0)
    low = lane < HALF
    causal = row >= lane
    lane1 = lax.broadcasted_iota(jnp.int32, (1, 128), 1)
    low1 = lane1 < HALF

    dtrow[...] = jnp.zeros_like(dtrow)
    for j in range(blocks):
        dtrow[j, 0:2, :] = dt_ref[:, j * BLOCK : (j + 1) * BLOCK].astype(F32)
    flat = (blocks * 8, 128)
    part = lax.rem(lax.broadcasted_iota(jnp.int32, flat, 0), 8)
    by_head = lambda ref: jnp.where(part == 0, ref[0], ref[1])
    raw = dtrow[...].reshape(flat) + by_head(bias_ref)
    rate = jnp.exp(by_head(alog_ref))
    dt = jnp.maximum(raw, 0.0) + jnp.log1p(jnp.exp(-jnp.abs(raw)))
    step = -dt * rate
    upto = (row <= lane).astype(F32)
    cum = mm_exact(step, upto)
    cum3 = cum.reshape(blocks, 8, 128)
    dt3 = dt.reshape(blocks, 8, 128)
    rowbuf[...] = jnp.where(
        lax.broadcasted_iota(jnp.int32, (blocks, 8, 128), 1) < 2, cum3, jnp.roll(dt3, 2, axis=1)
    )

    wx = taps_of(cx_ref)
    wb = taps_of(cb_ref, group_at)
    wc = taps_of(cc_ref, group_at)
    skip_e = jnp.where(low1, dskip_ref[0], dskip_ref[1])

    for i in range(4):
        loads[i].wait()

    tails[...] = jnp.zeros_like(tails)
    state[...] = jnp.zeros_like(state)

    def filtered(src, slot, taps, j):
        now = src[rows(j), :].astype(F32)
        window = jnp.concatenate([tails[slot], now], axis=0)
        tails[slot] = now[BLOCK - 8 :]
        total = now * taps[3]
        for k in range(3):
            total = total + window[5 + k : 5 + k + BLOCK] * taps[k]
        gate = sigmoid(total)
        act = total * gate
        return act, gate + act * (1.0 - gate)

    def halves(v):
        zero = jnp.zeros_like(v)
        return jnp.concatenate([jnp.where(low, v, zero), jnp.where(low, zero, v)], axis=0)

    def forward(j, carry):
        x_f, x_d = filtered(xv, 0, wx, j)
        b_f, b_d = filtered(bv, 1, wb, j)
        c_f, c_d = filtered(cv, 2, wc, j)
        at = rows(j)
        x_slope[at, :] = x_d
        b_p = split(b_f)
        c_p = split(c_f)
        b_act[at, :] = side(*b_p)
        b_slope[at, :] = b_d
        c_act[at, :] = side(*c_p)
        c_slope[at, :] = c_d
        own = rowbuf[j]
        columns = own.T
        cum_c0 = columns[:, 0:1]
        cum_c1 = columns[:, 1:2]
        dts = jnp.where(low, columns[:, 2:3], columns[:, 3:4])
        cums = jnp.where(low, cum_c0, cum_c1)
        dt_e[at, :] = dts
        cum_e[at, :] = cums
        l0 = jnp.where(causal, jnp.exp(jnp.minimum(cum_c0 - own[0:1], 0.0)), 0.0)
        l1 = jnp.where(causal, jnp.exp(jnp.minimum(cum_c1 - own[1:2], 0.0)), 0.0)
        decay0[at, :] = l0
        decay1[at, :] = l1
        sc = mm3(c_p, b_p, 1, 1)
        scores[at, :] = sc
        scaled = x_f * dts
        xs_hi, xs_lo = split(scaled)
        xs_buf[at, :] = side(xs_hi, xs_lo)
        last = cums[BLOCK - 1 : BLOCK]
        held = state[...]
        states[at, :] = held
        p0_hi, p0_lo = split(sc * l0)
        p1_hi, p1_lo = split(sc * l1)
        p_hi = side(p0_hi, p1_hi)
        p_lo = side(p0_lo, p1_lo)
        p_buf[at, :] = side(p_hi, p_lo)
        xs_h = halves(xs_hi)
        within = mm(p_hi, xs_h) + mm(p_lo, xs_h) + mm(p_hi, halves(xs_lo))
        brought = mm3(c_p, split(held), 1, 0) * jnp.exp(cums)
        carried_buf[at, :] = brought
        y_buf[at, :] = within + brought + skip_e * x_f
        ending = split(scaled * jnp.exp(last - cums))
        state[...] = held * jnp.exp(last) + mm3(b_p, ending, 0, 0)
        return carry

    lax.fori_loop(0, blocks, forward, 0, unroll=2)

    gain = nw_ref[...]
    segments = ((row < HALF) == low).astype(BF16)
    segments = jnp.concatenate([segments, segments], axis=0)

    def segment_mean(v):
        return mm(side(*split(v)), segments) * (1.0 / HALF)

    def gate_block(j):
        at = rows(j)
        y = y_buf[at, :]
        z = zv[at, :].astype(F32)
        gate = sigmoid(z)
        silz = z * gate
        gated = y * silz
        weighted = cotv[j].astype(F32) * gain
        inverse = lax.rsqrt(segment_mean(gated * gated) + EPS)
        mean2 = segment_mean(gated * weighted)
        d_gated = inverse * (weighted - gated * (inverse * inverse * mean2))
        dy = d_gated * silz
        dy_buf[at, :] = dy
        dz_send[j] = (d_gated * y * (gate + silz * (1.0 - gate))).astype(BF16)

        b_p = pair_at(b_act, at)
        c_p = pair_at(c_act, at)
        l0 = decay0[at, :]
        l1 = decay1[at, :]
        sc = scores[at, :]
        xs_hi, xs_lo = pair_at(xs_buf, at)
        dy_hi, dy_lo = split(dy)
        dy_hi = halves(dy_hi)
        dy_lo = halves(dy_lo)
        d_p = mm(side(dy_hi, dy_lo), side(xs_hi, xs_hi), ((1,), (1,))) + mm(
            dy_hi, xs_lo, ((1,), (1,))
        )
        d_p0 = d_p[:BLOCK]
        d_p1 = d_p[BLOCK:]
        d_sc = split(d_p0 * l0 + d_p1 * l1)
        m0 = d_p0 * (sc * l0)
        m1 = d_p1 * (sc * l1)
        p_hi = stack(*pair_at(p_buf, at))
        p_lo = stack(*pair_at(p_buf, at, 256))
        y_buf[at, :] = (
            mm(p_hi, dy_hi, ((0,), (0,)))
            + mm(p_lo, dy_hi, ((0,), (0,)))
            + mm(p_hi, dy_lo, ((0,), (0,)))
        )
        start = split(dy * jnp.exp(cum_e[at, :]))
        decay0[at, :] = mm3(c_p, start, 0, 0)
        decay1[at, :] = mm3(d_sc, c_p, 0, 0)
        d_c = mm3(d_sc, b_p, 1, 0) + mm3(start, split(states[at, :]), 1, 1)
        c_slope[at, :] = d_c * c_slope[at, :]
        diff = dy * carried_buf[at, :]
        zero = jnp.zeros_like(diff)
        col0 = jnp.sum(m0 + jnp.where(low, diff, zero), axis=1, keepdims=True)
        col1 = jnp.sum(m1 + jnp.where(low, zero, diff), axis=1, keepdims=True)
        turned = jnp.where(lane == 0, col0, col1).T[0:8]
        dcumbuf[j, 0:1, :] = turned[0:1] - jnp.sum(m0, axis=0, keepdims=True)
        dcumbuf[j, 1:2, :] = turned[1:2] - jnp.sum(m1, axis=0, keepdims=True)

    def columns_of(ref, i):
        return ref.at[:, pl.ds(pl.multiple_of(i * 128, 128), 128)]

    def grad_copy(buf, out, s_sem, r_sem, peer, slot):
        return to(buf.at[peer], columns_of(out, slot), s_sem.at[peer], r_sem.at[slot], peer, seq)

    dcumbuf[...] = jnp.zeros_like(dcumbuf)
    rbuf[...] = jnp.zeros_like(rbuf)
    beside = behind(1)
    loads[5].wait()
    cot_copy(me, beside).wait_recv()
    gate_block(me)
    gate_block(beside)
    dz_own = pltpu.make_async_copy(dz_send.at[me], columns_of(dz_out, me), loc.at[6])
    dz_own.start()

    def send_dz(o):
        grad_copy(dz_send, dz_out, dz_s, dz_r, behind(o), me).start()

    send_dz(1)

    def gate_pair(p, send):
        o = 2 * p
        first = behind(o)
        second = behind(o + 1)
        cot_copy(me, first).wait_recv()
        cot_copy(me, second).wait_recv()
        gate_block(first)
        gate_block(second)
        if send:
            send_dz(o)
            send_dz(o + 1)

    early = min(DZ_EARLY, n_sp // 2)
    some(1, early, lambda p: gate_pair(p, True))
    some(early, n_sp // 2, lambda p: gate_pair(p, False))
    early = 2 * early

    state[...] = jnp.zeros_like(state)

    def enter(i, carry):
        j = blocks - 1 - i
        at = rows(j)
        grad = state[...]
        own = decay0[at, :]
        decay0[at, :] = grad
        end = pl.ds(pl.multiple_of(j * BLOCK + BLOCK - 8, 8), 8)
        state[...] = grad * jnp.exp(cum_e[end, :][7:8]) + own
        return carry

    lax.fori_loop(0, blocks, enter, 0)

    tails[...] = jnp.zeros_like(tails)

    def unfiltered(d, slot, taps):
        window = jnp.concatenate([d, tails[slot]], axis=0)
        tails[slot] = d[0:8]
        total = d * taps[3]
        for k in range(3):
            total = total + window[3 - k : 3 - k + BLOCK] * taps[k]
        return total

    def backward(j, carry):
        at = rows(j)
        cums = cum_e[at, :]
        xs_hi, xs_lo = pair_at(xs_buf, at)
        scaled = xs_hi.astype(F32) + xs_lo.astype(F32)
        last = cums[BLOCK - 1 : BLOCK]
        to_end = jnp.exp(last - cums)
        grad = decay0[at, :]
        reached = mm3(pair_at(b_act, at), split(grad), 1, 0) * to_end
        d_scaled = y_buf[at, :] + reached
        x_slope[at, :] = (d_scaled * dt_e[at, :] + skip_e * dy_buf[at, :]) * x_slope[at, :]
        kept = reached * scaled
        direct = d_scaled * scaled
        zero = jnp.zeros_like(kept)
        col0 = jnp.sum(jnp.where(low, kept, zero), axis=1, keepdims=True)
        col1 = jnp.sum(jnp.where(low, zero, kept), axis=1, keepdims=True)
        col2 = jnp.sum(jnp.where(low, direct, zero), axis=1, keepdims=True)
        col3 = jnp.sum(jnp.where(low, zero, direct), axis=1, keepdims=True)
        turned = jnp.where(
            lane == 0, col0, jnp.where(lane == 1, col1, jnp.where(lane == 2, col2, col3))
        ).T[0:8]
        ends = jnp.sum(kept, axis=0, keepdims=True) + jnp.exp(last) * jnp.sum(
            grad * states[at, :], axis=0, keepdims=True
        )
        end0 = jnp.sum(jnp.where(low1, ends, 0.0), axis=1, keepdims=True)
        end1 = jnp.sum(jnp.where(low1, 0.0, ends), axis=1, keepdims=True)
        at_end = lane1 == BLOCK - 1
        dcumbuf[j, 0:1, :] = dcumbuf[j, 0:1, :] + jnp.where(at_end, end0, 0.0) - turned[0:1]
        dcumbuf[j, 1:2, :] = dcumbuf[j, 1:2, :] + jnp.where(at_end, end1, 0.0) - turned[1:2]
        rbuf[j, 0:2, :] = turned[2:4]
        return carry

    lax.fori_loop(0, blocks, backward, 0, unroll=4)

    since = (row >= lane).astype(F32)
    d_step = mm_exact(dcumbuf[...].reshape(flat), since)
    raw = dtrow[...].reshape(flat) + by_head(bias_ref)
    d_dt = rbuf[...].reshape(flat) / dt - d_step * rate
    d_raw = jnp.where(part < 2, d_dt * sigmoid(raw), 0.0)
    ddt_tx[...] = d_raw.astype(BF16).astype(F32).reshape(blocks, 8, 128)
    ga_part = jnp.sum((d_step * step).reshape(blocks, 8, 128), axis=0)

    def ddt_copy(peer, slot):
        return to(ddt_tx.at[peer], ddt_rx.at[slot], ddt_s.at[peer], ddt_r.at[slot], peer, seq)

    each(n_sp, lambda o: ddt_copy(ahead(o), me).start())
    some(early, n_sp, send_dz)

    def filters(i, carry):
        j = blocks - 1 - i
        at = rows(j)
        cums = cum_e[at, :]
        xs_hi, xs_lo = pair_at(xs_buf, at)
        ending = (xs_hi.astype(F32) + xs_lo.astype(F32)) * jnp.exp(cums[BLOCK - 1 : BLOCK] - cums)
        d_b = decay1[at, :] + mm3(split(ending), split(decay0[at, :]), 1, 1)
        dx_send[j] = unfiltered(x_slope[at, :], 0, wx).astype(BF16)
        bc_send[j, :, 0:STATE] = unfiltered(d_b * b_slope[at, :], 1, wb).astype(BF16)
        bc_send[j, :, STATE:] = unfiltered(c_slope[at, :], 2, wc).astype(BF16)
        return carry

    lax.fori_loop(0, blocks, filters, 0, unroll=2)
    partner = me + 1 - 2 * core
    pair_copies = lambda q: to(
        bc_send.at[2 * q + 1 - core], pair_rx.at[q], pair_s.at[q], pair_r.at[q], partner, seq
    )
    some(0, chips, lambda q: pair_copies(q).start())

    def send_dx(o):
        grad_copy(dx_send, dx_out, dx_s, dx_r, ahead(o), me).start()

    dx_early = min(DX_EARLY, n_sp - 1) + 1
    some(1, dx_early, send_dx)
    dx_own = pltpu.make_async_copy(dx_send.at[me], columns_of(dx_out, me), loc.at[7])
    dx_own.start()
    ddt_rx[me] = ddt_tx[me]
    each(n_sp, lambda o: ddt_copy(me, wrap(me + o, n_sp)).wait_recv())

    heads = 2 * n_sp
    source = lax.broadcasted_iota(jnp.int32, (heads, blocks * 8), 1)
    target = lax.broadcasted_iota(jnp.int32, (heads, blocks * 8), 0)
    pick = (source == (target // 2) * 8 + lax.rem(target, 2)).astype(BF16)
    own_ddt = mm(pick, ddt_rx[...].reshape(flat).astype(BF16)).astype(BF16)
    ddt_out[...] = own_ddt
    loads[4].wait()
    per_row = liv.shape[1] // 128

    ga_sum = jnp.broadcast_to(jnp.sum(ga_part, axis=1, keepdims=True), (8, 128))
    ga_tx[0] = ga_sum
    for c0 in range(0, per_row, 4):
        piece = mm(own_ddt, liv[:, c0 * 128 : (c0 + 4) * 128])
        for r in range(heads // 8):
            for c in range(4):
                t = r * per_row + c0 + c
                tile = piece[8 * r : 8 * r + 8, c * 128 : (c + 1) * 128]
                at = (t % w_tiles) * 8
                w_tx[t // w_tiles, at : at + 8, :] = tile.astype(BF16)

    def scatter_copy(k, slot):
        return to(w_tx.at[k], w_rx.at[slot], f_s.at[k], f_r.at[slot], me, k)

    each(n_dp, lambda o: scatter_copy(wrap(seq + hop(o, n_dp), n_dp), seq).start())

    n_edge = math.isqrt(n_dp)
    z_at = seq // n_edge
    y_at = lax.rem(seq, n_edge)

    def y_copy(k, slot):
        dst = ga_rx.at[0, slot]
        return to(ga_tx.at[0], dst, ga_s.at[0, k], ga_r.at[0, slot], me, z_at * n_edge + k)

    def z_copy(k, slot):
        dst = ga_rx.at[1, slot]
        return to(ga_tx.at[1], dst, ga_s.at[1, k], ga_r.at[1, slot], me, k * n_edge + y_at)

    each(n_edge, lambda o: y_copy(wrap(y_at + o, n_edge), y_at).start())

    def pair_add(q, c):
        pair_copies(q).wait_recv()
        mine = bc_send[2 * q + core].astype(F32)
        bc_sum[q] = (mine + pair_rx[q].astype(F32)).astype(BF16)
        return c

    lax.fori_loop(0, chips, pair_add, 0)

    w_rx[seq] = w_tx[seq]
    each(n_dp, lambda o: scatter_copy(seq, wrap(seq + o, n_dp)).wait_recv())
    sum2 = lax.fori_loop(
        1, n_dp, lambda k, t: t + w_rx[k].astype(F32), w_rx[0].astype(F32), unroll=3 if n_dp == 64 else 1
    )
    u_tx[...] = sum2

    def sp_copy(peer, slot):
        return to(u_tx, u_rx.at[slot], h_s.at[peer], h_r.at[slot], peer, seq)

    each(n_sp, lambda o: sp_copy(ahead(o), me).start())

    def bc_copy(q, slot):
        return to(bc_sum.at[q], bc_rx.at[slot], bc_s.at[q], bc_r.at[slot], 2 * q + core, seq)

    some(dx_early, n_sp, send_dx)
    each(chips, lambda o: bc_copy(wrap(chip + hop(o, chips), chips), chip).start())

    def summed(a):
        total = ga_rx[a, 0]
        for k in range(1, n_edge):
            total = total + ga_rx[a, k]
        return total

    ga_rx[0, y_at] = ga_tx[0]
    each(n_edge, lambda o: y_copy(y_at, wrap(y_at + o, n_edge)).wait_recv())
    ga_tx[1] = summed(0)
    each(n_edge, lambda o: z_copy(wrap(z_at + o, n_edge), z_at).start())
    ga_rx[1, z_at] = ga_tx[1]

    u_rx[me] = u_tx[...]
    each(n_sp, lambda o: sp_copy(me, wrap(me + o, n_sp)).wait_recv())
    sum3 = u_rx[0]
    for k in range(1, n_sp):
        sum3 = sum3 + u_rx[k]
    w_fin[seq] = sum3.astype(BF16)

    def gather_copy(k, slot):
        return to(w_fin.at[slot], w_fin.at[slot], k_s.at[k], k_r.at[slot], me, k)

    each(n_dp, lambda o: gather_copy(wrap(seq + hop(o, n_dp), n_dp), seq).start())

    each(n_edge, lambda o: z_copy(z_at, wrap(z_at + o, n_edge)).wait_recv())
    ga_out[...] = summed(1)

    bc_rx[chip] = bc_sum[chip]
    each(chips, lambda o: bc_copy(chip, wrap(chip + o, chips)).wait_recv())
    span = chips // GROUPS
    for g in range(GROUPS):
        total = bc_rx[g * span].astype(F32)
        for q in range(1, span):
            total = total + bc_rx[g * span + q].astype(F32)
        db_out[:, g * STATE : (g + 1) * STATE] = total[:, 0:STATE].astype(BF16)
        dc_out[:, g * STATE : (g + 1) * STATE] = total[:, STATE:].astype(BF16)

    def finish(o):
        peer = wrap(me + o, n_sp)
        cot_copy(peer, me).wait_send()
        ddt_copy(peer, me).wait_send()
        sp_copy(peer, me).wait_send()
        dz = grad_copy(dz_send, dz_out, dz_s, dz_r, peer, me)
        dz.wait_send()
        grad_copy(dz_send, dz_out, dz_s, dz_r, me, peer).wait_recv()
        grad_copy(dx_send, dx_out, dx_s, dx_r, peer, me).wait_send()
        grad_copy(dx_send, dx_out, dx_s, dx_r, me, peer).wait_recv()

    each(n_sp, finish)
    lax.fori_loop(0, chips, lambda q, c: (pair_copies(q).wait_send(), c)[1], 0)
    each(chips, lambda o: bc_copy(wrap(chip + o, chips), chip).wait_send())

    def finish_seq(o):
        peer = wrap(seq + o, n_dp)
        scatter_copy(peer, seq).wait_send()
        gather_copy(peer, seq).wait_send()
        gather_copy(seq, peer).wait_recv()

    each(n_dp, finish_seq)
    each(n_edge, lambda o: y_copy(wrap(y_at + o, n_edge), y_at).wait_send())
    each(n_edge, lambda o: z_copy(wrap(z_at + o, n_edge), z_at).wait_send())
    dz_own.wait()
    dx_own.wait()


def mixer(n_sp, n_dp, *args):
    n_edge = math.isqrt(n_dp)
    chips = n_sp // 2
    blocks = n_sp
    length = blocks * BLOCK
    width = n_sp * 128
    model = args[1].shape[1]
    heads = 2 * n_sp
    tiles = (heads // 8) * (model // 128)
    w_rows = 8 * tiles // n_dp
    any_space = pl.BlockSpec(memory_space=pl.ANY)
    vmem = pl.BlockSpec(memory_space=pltpu.VMEM)
    smem = pl.BlockSpec(memory_space=pltpu.SMEM)
    V = pltpu.VMEM
    seq_f = V((length, 128), F32)
    seq_b = V((length, 128), BF16)
    seq_d = V((length, 256), BF16)
    blk_b = V((blocks, BLOCK, 128), BF16)
    dma = lambda n: pltpu.SemaphoreType.DMA((n,))
    parts = pl.pallas_call(
        functools.partial(kernel, n_sp, n_dp),
        out_shape=(
            jax.ShapeDtypeStruct((BLOCK, width), BF16),
            jax.ShapeDtypeStruct((BLOCK, width), BF16),
            jax.ShapeDtypeStruct((BLOCK, GROUPS * STATE), BF16),
            jax.ShapeDtypeStruct((BLOCK, GROUPS * STATE), BF16),
            jax.ShapeDtypeStruct((heads, BLOCK), BF16),
            jax.ShapeDtypeStruct((8, 128), F32),
            jax.ShapeDtypeStruct((n_dp, w_rows, 128), BF16),
        ),
        in_specs=[any_space] * 6 + [vmem] * 5 + [smem] * 3,
        out_specs=(any_space, any_space) + (vmem,) * 5,
        scratch_shapes=[
            seq_b,
            seq_b,
            seq_b,
            seq_b,
            V((BLOCK, model), BF16),
            blk_b,
            V((blocks, 8, 128), F32),
            V((blocks, 8, 128), F32),
            V((blocks, 8, 128), F32),
            V((blocks, 8, 128), F32),
            seq_f,
            seq_d,
            seq_f,
            seq_d,
            seq_f,
            seq_f,
            seq_f,
            seq_f,
            V((length, 4 * BLOCK), BF16),
            seq_d,
            seq_f,
            seq_f,
            seq_f,
            seq_f,
            seq_f,
            seq_f,
            V((STATE, 128), F32),
            V((3, 8, 128), F32),
            blk_b,
            blk_b,
            V((blocks, BLOCK, 2 * STATE), BF16),
            V((chips, BLOCK, 2 * STATE), BF16),
            V((chips, BLOCK, 2 * STATE), BF16),
            V((chips, BLOCK, 2 * STATE), BF16),
            V((blocks, 8, 128), F32),
            V((blocks, 8, 128), F32),
            V((n_dp, w_rows, 128), BF16),
            V((n_dp, w_rows, 128), BF16),
            V((w_rows, 128), F32),
            V((n_sp, w_rows, 128), F32),
            V((2, 8, 128), F32),
            V((2, n_edge, 8, 128), F32),
            dma(8),
            dma(n_sp),
            dma(n_sp),
            dma(n_sp),
            dma(n_sp),
            dma(n_sp),
            dma(n_sp),
            dma(n_sp),
            dma(n_sp),
            dma(chips),
            dma(chips),
            dma(chips),
            dma(chips),
            dma(n_dp),
            dma(n_dp),
            dma(n_sp),
            dma(n_sp),
            dma(n_dp),
            dma(n_dp),
            pltpu.SemaphoreType.DMA((2, n_edge)),
            pltpu.SemaphoreType.DMA((2, n_edge)),
        ],
        compiler_params=pltpu.CompilerParams(
            collective_id=0, has_side_effects=True, vmem_limit_bytes=60000 * 1024
        ),
        name="mixer_backward",
    )(*args)
    return pl.pallas_call(
        finish_kernel,
        out_shape=tuple(jax.ShapeDtypeStruct(p.shape, p.dtype) for p in parts[:5])
        + (jax.ShapeDtypeStruct((2,), F32), jax.ShapeDtypeStruct((heads, model), F32)),
        in_specs=[vmem] * 7,
        out_specs=(vmem,) * 5 + (smem, vmem),
        name="finish",
    )(*parts)


def finish_kernel(dx, dz, db, dc, ddt, ga, w, dx_out, dz_out, db_out, dc_out, ddt_out, ga_out, gw_out):
    dx_out[...] = dx[...]
    dz_out[...] = dz[...]
    db_out[...] = db[...]
    dc_out[...] = dc[...]
    ddt_out[...] = ddt[...]
    ga_out[0] = ga[0, 0]
    ga_out[1] = ga[1, 0]
    per_row = gw_out.shape[1] // 128
    w_tiles = w.shape[1] // 8
    for t in range(w.shape[0] * w_tiles):
        r, c, at = t // per_row, t % per_row, 8 * (t % w_tiles)
        gw_out[8 * r : 8 * r + 8, c * 128 : (c + 1) * 128] = w[t // w_tiles, at : at + 8, :].astype(F32)


def shards(
    n_sp,
    n_dp,
    cotangent,
    layer_input,
    x_pre,
    z_pre,
    b_pre,
    c_pre,
    dt_raw,
    conv_x,
    conv_b,
    conv_c,
    dt_bias,
    a_log,
    d_skip,
    norm_w,
):
    dx, dz, db, dc, ddt, ga, gw = mixer(
        n_sp,
        n_dp,
        cotangent[0],
        layer_input[0],
        x_pre[0],
        z_pre[0],
        b_pre[0],
        c_pre[0],
        dt_raw[0].T,
        conv_x,
        conv_b,
        conv_c,
        norm_w[None],
        dt_bias,
        a_log,
        d_skip,
    )
    return (dx[None], dz[None], db[None], dc[None], ddt.T[None], ga, gw.T)


def solution(mesh):
    in_specs = (
        P("dp", "sp", None),
        P("dp", "sp", None),
        P("dp", None, "sp"),
        P("dp", None, "sp"),
        P("dp", None, None),
        P("dp", None, None),
        P("dp", None, "sp"),
        P(None, "sp"),
        P(),
        P(),
        P("sp"),
        P("sp"),
        P("sp"),
        P("sp"),
    )
    out_specs = (
        P("dp", "sp", None),
        P("dp", "sp", None),
        P("dp", "sp", None),
        P("dp", "sp", None),
        P("dp", "sp", None),
        P("sp"),
        P(),
    )
    return jax.shard_map(
        functools.partial(shards, mesh.shape["sp"], mesh.shape["dp"]),
        mesh=mesh,
        in_specs=in_specs,
        out_specs=out_specs,
        check_vma=False,
    )
```

```python
import functools
import math

import jax
import jax.numpy as jnp
from jax import lax
from jax.experimental import pallas as pl
from jax.experimental.pallas import tpu as pltpu
from jax.sharding import PartitionSpec as P

GROUPS = 2
STATE = 128
BLOCK = 128
TAPS = 4
HALF = 64
EPS = 1e-05
DZ_EARLY = 8
DX_EARLY = 15
F32 = jnp.float32
BF16 = jnp.bfloat16


def mm(a, b, dims=((1,), (0,))):
    return lax.dot_general(a, b, (dims, ((), ())), preferred_element_type=F32)


def mm_exact(a, b):
    return lax.dot_general(
        a, b, (((1,), (0,)), ((), ())), precision=lax.Precision.HIGHEST, preferred_element_type=F32
    )


def split(v):
    high = v.astype(BF16)
    return high, (v - high.astype(F32)).astype(BF16)


def side(*parts):
    return jnp.concatenate(parts, axis=1)


def stack(*parts):
    return jnp.concatenate(parts, axis=0)


def mm3(a, b, ca, cb):
    join_a = side if ca else stack
    join_b = side if cb else stack
    dims = ((ca,), (cb,))
    return mm(join_a(*a), join_b(b[0], b[0]), dims) + mm(a[0], b[1], dims)


def pair_at(ref, at, start=0):
    return ref[at, start : start + 128], ref[at, start + 128 : start + 256]


def sigmoid(v):
    return 1.0 / (1.0 + jnp.exp(-v))


def taps_of(ref, start=None):
    whole = ref[...] if start is None else ref[:, pl.ds(start, 128)]
    whole = whole.astype(F32)
    return [whole[k : k + 1] for k in range(TAPS)]


def rows(j):
    return pl.ds(pl.multiple_of(j * BLOCK, BLOCK), BLOCK)


def kernel(
    n_sp,
    n_dp,
    cot_hbm,
    li_hbm,
    x_hbm,
    z_hbm,
    b_hbm,
    c_hbm,
    dt_ref,
    cx_ref,
    cb_ref,
    cc_ref,
    nw_ref,
    bias_ref,
    alog_ref,
    dskip_ref,
    dx_out,
    dz_out,
    db_out,
    dc_out,
    ddt_out,
    ga_out,
    w_fin,
    xv,
    zv,
    bv,
    cv,
    liv,
    cotv,
    dtrow,
    rowbuf,
    dcumbuf,
    rbuf,
    x_slope,
    b_act,
    b_slope,
    c_act,
    c_slope,
    decay0,
    decay1,
    scores,
    p_buf,
    xs_buf,
    y_buf,
    carried_buf,
    dy_buf,
    dt_e,
    cum_e,
    states,
    state,
    tails,
    dz_send,
    dx_send,
    bc_send,
    pair_rx,
    bc_sum,
    bc_rx,
    ddt_tx,
    ddt_rx,
    w_tx,
    w_rx,
    u_tx,
    u_rx,
    ga_tx,
    ga_rx,
    loc,
    cot_s,
    cot_r,
    dz_s,
    dz_r,
    dx_s,
    dx_r,
    ddt_s,
    ddt_r,
    bc_s,
    bc_r,
    pair_s,
    pair_r,
    f_s,
    f_r,
    h_s,
    h_r,
    k_s,
    k_r,
    ga_s,
    ga_r,
):
    blocks = n_sp
    chips = n_sp // 2
    w_rows = w_fin.shape[1]
    w_tiles = w_rows // 8
    me = lax.axis_index("sp")
    seq = lax.axis_index("dp")
    core = lax.rem(me, 2)
    chip = me // 2
    group = me // (n_sp // GROUPS)
    group_at = pl.multiple_of(group * STATE, STATE)

    def wrap(i, n):
        return lax.rem(i + n, n)

    def hop(p, n):
        odd = p % 2 if isinstance(p, int) else lax.rem(p, 2)
        return ((p + 1) // 2) * odd + (n - p // 2) * (1 - odd)

    def ahead(p):
        return wrap(me + hop(p, n_sp), n_sp)

    def behind(p):
        return wrap(me - hop(p, n_sp), n_sp)

    def to(src, dst, s_sem, r_sem, sp, dp):
        return pltpu.make_async_remote_copy(
            src_ref=src,
            dst_ref=dst,
            send_sem=s_sem,
            recv_sem=r_sem,
            device_id={"sp": sp, "dp": dp},
            device_id_type=pl.DeviceIdType.MESH,
        )

    def each(n, body):
        if n > 1:
            lax.fori_loop(1, n, lambda o, c: (body(o), c)[1], 0)

    def some(low_o, high_o, body):
        lax.fori_loop(low_o, high_o, lambda o, c: (body(o), c)[1], 0)

    loads = [
        pltpu.make_async_copy(x_hbm, xv, loc.at[0]),
        pltpu.make_async_copy(b_hbm.at[:, pl.ds(group_at, STATE)], bv, loc.at[1]),
        pltpu.make_async_copy(c_hbm.at[:, pl.ds(group_at, STATE)], cv, loc.at[2]),
        pltpu.make_async_copy(z_hbm, zv, loc.at[3]),
        pltpu.make_async_copy(li_hbm, liv, loc.at[4]),
        pltpu.make_async_copy(
            cot_hbm.at[:, pl.ds(pl.multiple_of(me * 128, 128), 128)], cotv.at[me], loc.at[5]
        ),
    ]
    for load in loads:
        load.start()

    barrier = pltpu.get_barrier_semaphore()

    def greet(sp, dp):
        pl.semaphore_signal(
            barrier, inc=1, device_id={"sp": sp, "dp": dp}, device_id_type=pl.DeviceIdType.MESH
        )

    each(n_sp, lambda o: greet(wrap(me + o, n_sp), seq))
    each(n_dp, lambda o: greet(me, wrap(seq + o, n_dp)))
    def cot_copy(peer, slot):
        return to(
            cot_hbm.at[:, pl.ds(pl.multiple_of(peer * 128, 128), 128)],
            cotv.at[slot],
            cot_s.at[peer],
            cot_r.at[slot],
            peer,
            seq,
        )

    pl.semaphore_wait(barrier, (n_sp - 1) + (n_dp - 1))
    each(n_sp, lambda o: cot_copy(ahead(o), me).start())

    lane = lax.broadcasted_iota(jnp.int32, (BLOCK, 128), 1)
    row = lax.broadcasted_iota(jnp.int32, (BLOCK, 128), 0)
    low = lane < HALF
    causal = row >= lane
    lane1 = lax.broadcasted_iota(jnp.int32, (1, 128), 1)
    low1 = lane1 < HALF

    dtrow[...] = jnp.zeros_like(dtrow)
    for j in range(blocks):
        dtrow[j, 0:2, :] = dt_ref[:, j * BLOCK : (j + 1) * BLOCK].astype(F32)
    flat = (blocks * 8, 128)
    part = lax.rem(lax.broadcasted_iota(jnp.int32, flat, 0), 8)
    by_head = lambda ref: jnp.where(part == 0, ref[0], ref[1])
    raw = dtrow[...].reshape(flat) + by_head(bias_ref)
    rate = jnp.exp(by_head(alog_ref))
    dt = jnp.maximum(raw, 0.0) + jnp.log1p(jnp.exp(-jnp.abs(raw)))
    step = -dt * rate
    upto = (row <= lane).astype(F32)
    cum = mm_exact(step, upto)
    cum3 = cum.reshape(blocks, 8, 128)
    dt3 = dt.reshape(blocks, 8, 128)
    rowbuf[...] = jnp.where(
        lax.broadcasted_iota(jnp.int32, (blocks, 8, 128), 1) < 2, cum3, jnp.roll(dt3, 2, axis=1)
    )

    wx = taps_of(cx_ref)
    wb = taps_of(cb_ref, group_at)
    wc = taps_of(cc_ref, group_at)
    skip_e = jnp.where(low1, dskip_ref[0], dskip_ref[1])

    for i in range(4):
        loads[i].wait()

    tails[...] = jnp.zeros_like(tails)
    state[...] = jnp.zeros_like(state)

    def filtered(src, slot, taps, j):
        now = src[rows(j), :].astype(F32)
        window = jnp.concatenate([tails[slot], now], axis=0)
        tails[slot] = now[BLOCK - 8 :]
        total = now * taps[3]
        for k in range(3):
            total = total + window[5 + k : 5 + k + BLOCK] * taps[k]
        gate = sigmoid(total)
        act = total * gate
        return act, gate + act * (1.0 - gate)

    def halves(v):
        zero = jnp.zeros_like(v)
        return jnp.concatenate([jnp.where(low, v, zero), jnp.where(low, zero, v)], axis=0)

    def forward(j, carry):
        x_f, x_d = filtered(xv, 0, wx, j)
        b_f, b_d = filtered(bv, 1, wb, j)
        c_f, c_d = filtered(cv, 2, wc, j)
        at = rows(j)
        x_slope[at, :] = x_d
        b_p = split(b_f)
        c_p = split(c_f)
        b_act[at, :] = side(*b_p)
        b_slope[at, :] = b_d
        c_act[at, :] = side(*c_p)
        c_slope[at, :] = c_d
        own = rowbuf[j]
        columns = own.T
        cum_c0 = columns[:, 0:1]
        cum_c1 = columns[:, 1:2]
        dts = jnp.where(low, columns[:, 2:3], columns[:, 3:4])
        cums = jnp.where(low, cum_c0, cum_c1)
        dt_e[at, :] = dts
        cum_e[at, :] = cums
        l0 = jnp.where(causal, jnp.exp(jnp.minimum(cum_c0 - own[0:1], 0.0)), 0.0)
        l1 = jnp.where(causal, jnp.exp(jnp.minimum(cum_c1 - own[1:2], 0.0)), 0.0)
        decay0[at, :] = l0
        decay1[at, :] = l1
        sc = mm3(c_p, b_p, 1, 1)
        scores[at, :] = sc
        scaled = x_f * dts
        xs_hi, xs_lo = split(scaled)
        xs_buf[at, :] = side(xs_hi, xs_lo)
        last = cums[BLOCK - 1 : BLOCK]
        held = state[...]
        states[at, :] = held
        p0_hi, p0_lo = split(sc * l0)
        p1_hi, p1_lo = split(sc * l1)
        p_hi = side(p0_hi, p1_hi)
        p_lo = side(p0_lo, p1_lo)
        p_buf[at, :] = side(p_hi, p_lo)
        xs_h = halves(xs_hi)
        within = mm(p_hi, xs_h) + mm(p_lo, xs_h) + mm(p_hi, halves(xs_lo))
        brought = mm3(c_p, split(held), 1, 0) * jnp.exp(cums)
        carried_buf[at, :] = brought
        y_buf[at, :] = within + brought + skip_e * x_f
        ending = split(scaled * jnp.exp(last - cums))
        state[...] = held * jnp.exp(last) + mm3(b_p, ending, 0, 0)
        return carry

    lax.fori_loop(0, blocks, forward, 0, unroll=2)

    gain = nw_ref[...]
    segments = ((row < HALF) == low).astype(BF16)
    segments = jnp.concatenate([segments, segments], axis=0)

    def segment_mean(v):
        return mm(side(*split(v)), segments) * (1.0 / HALF)

    def gate_block(j):
        at = rows(j)
        y = y_buf[at, :]
        z = zv[at, :].astype(F32)
        gate = sigmoid(z)
        silz = z * gate
        gated = y * silz
        weighted = cotv[j].astype(F32) * gain
        inverse = lax.rsqrt(segment_mean(gated * gated) + EPS)
        mean2 = segment_mean(gated * weighted)
        d_gated = inverse * (weighted - gated * (inverse * inverse * mean2))
        dy = d_gated * silz
        dy_buf[at, :] = dy
        dz_send[j] = (d_gated * y * (gate + silz * (1.0 - gate))).astype(BF16)

        b_p = pair_at(b_act, at)
        c_p = pair_at(c_act, at)
        l0 = decay0[at, :]
        l1 = decay1[at, :]
        sc = scores[at, :]
        xs_hi, xs_lo = pair_at(xs_buf, at)
        dy_hi, dy_lo = split(dy)
        dy_hi = halves(dy_hi)
        dy_lo = halves(dy_lo)
        d_p = mm(side(dy_hi, dy_lo), side(xs_hi, xs_hi), ((1,), (1,))) + mm(
            dy_hi, xs_lo, ((1,), (1,))
        )
        d_p0 = d_p[:BLOCK]
        d_p1 = d_p[BLOCK:]
        d_sc = split(d_p0 * l0 + d_p1 * l1)
        m0 = d_p0 * (sc * l0)
        m1 = d_p1 * (sc * l1)
        p_hi = stack(*pair_at(p_buf, at))
        p_lo = stack(*pair_at(p_buf, at, 256))
        y_buf[at, :] = (
            mm(p_hi, dy_hi, ((0,), (0,)))
            + mm(p_lo, dy_hi, ((0,), (0,)))
            + mm(p_hi, dy_lo, ((0,), (0,)))
        )
        start = split(dy * jnp.exp(cum_e[at, :]))
        decay0[at, :] = mm3(c_p, start, 0, 0)
        decay1[at, :] = mm3(d_sc, c_p, 0, 0)
        d_c = mm3(d_sc, b_p, 1, 0) + mm3(start, split(states[at, :]), 1, 1)
        c_slope[at, :] = d_c * c_slope[at, :]
        diff = dy * carried_buf[at, :]
        zero = jnp.zeros_like(diff)
        col0 = jnp.sum(m0 + jnp.where(low, diff, zero), axis=1, keepdims=True)
        col1 = jnp.sum(m1 + jnp.where(low, zero, diff), axis=1, keepdims=True)
        turned = jnp.where(lane == 0, col0, col1).T[0:8]
        dcumbuf[j, 0:1, :] = turned[0:1] - jnp.sum(m0, axis=0, keepdims=True)
        dcumbuf[j, 1:2, :] = turned[1:2] - jnp.sum(m1, axis=0, keepdims=True)

    def columns_of(ref, i):
        return ref.at[:, pl.ds(pl.multiple_of(i * 128, 128), 128)]

    def grad_copy(buf, out, s_sem, r_sem, peer, slot):
        return to(buf.at[peer], columns_of(out, slot), s_sem.at[peer], r_sem.at[slot], peer, seq)

    dcumbuf[...] = jnp.zeros_like(dcumbuf)
    rbuf[...] = jnp.zeros_like(rbuf)
    beside = behind(1)
    loads[5].wait()
    cot_copy(me, beside).wait_recv()
    gate_block(me)
    gate_block(beside)
    dz_own = pltpu.make_async_copy(dz_send.at[me], columns_of(dz_out, me), loc.at[6])
    dz_own.start()

    def send_dz(o):
        grad_copy(dz_send, dz_out, dz_s, dz_r, behind(o), me).start()

    send_dz(1)

    def gate_pair(p, send):
        o = 2 * p
        first = behind(o)
        second = behind(o + 1)
        cot_copy(me, first).wait_recv()
        cot_copy(me, second).wait_recv()
        gate_block(first)
        gate_block(second)
        if send:
            send_dz(o)
            send_dz(o + 1)

    early = min(DZ_EARLY, n_sp // 2)
    some(1, early, lambda p: gate_pair(p, True))
    some(early, n_sp // 2, lambda p: gate_pair(p, False))
    early = 2 * early

    state[...] = jnp.zeros_like(state)

    def enter(i, carry):
        j = blocks - 1 - i
        at = rows(j)
        grad = state[...]
        own = decay0[at, :]
        decay0[at, :] = grad
        end = pl.ds(pl.multiple_of(j * BLOCK + BLOCK - 8, 8), 8)
        state[...] = grad * jnp.exp(cum_e[end, :][7:8]) + own
        return carry

    lax.fori_loop(0, blocks, enter, 0)

    tails[...] = jnp.zeros_like(tails)

    def unfiltered(d, slot, taps):
        window = jnp.concatenate([d, tails[slot]], axis=0)
        tails[slot] = d[0:8]
        total = d * taps[3]
        for k in range(3):
            total = total + window[3 - k : 3 - k + BLOCK] * taps[k]
        return total

    def backward(j, carry):
        at = rows(j)
        cums = cum_e[at, :]
        xs_hi, xs_lo = pair_at(xs_buf, at)
        scaled = xs_hi.astype(F32) + xs_lo.astype(F32)
        last = cums[BLOCK - 1 : BLOCK]
        to_end = jnp.exp(last - cums)
        grad = decay0[at, :]
        reached = mm3(pair_at(b_act, at), split(grad), 1, 0) * to_end
        d_scaled = y_buf[at, :] + reached
        x_slope[at, :] = (d_scaled * dt_e[at, :] + skip_e * dy_buf[at, :]) * x_slope[at, :]
        kept = reached * scaled
        direct = d_scaled * scaled
        zero = jnp.zeros_like(kept)
        col0 = jnp.sum(jnp.where(low, kept, zero), axis=1, keepdims=True)
        col1 = jnp.sum(jnp.where(low, zero, kept), axis=1, keepdims=True)
        col2 = jnp.sum(jnp.where(low, direct, zero), axis=1, keepdims=True)
        col3 = jnp.sum(jnp.where(low, zero, direct), axis=1, keepdims=True)
        turned = jnp.where(
            lane == 0, col0, jnp.where(lane == 1, col1, jnp.where(lane == 2, col2, col3))
        ).T[0:8]
        ends = jnp.sum(kept, axis=0, keepdims=True) + jnp.exp(last) * jnp.sum(
            grad * states[at, :], axis=0, keepdims=True
        )
        end0 = jnp.sum(jnp.where(low1, ends, 0.0), axis=1, keepdims=True)
        end1 = jnp.sum(jnp.where(low1, 0.0, ends), axis=1, keepdims=True)
        at_end = lane1 == BLOCK - 1
        dcumbuf[j, 0:1, :] = dcumbuf[j, 0:1, :] + jnp.where(at_end, end0, 0.0) - turned[0:1]
        dcumbuf[j, 1:2, :] = dcumbuf[j, 1:2, :] + jnp.where(at_end, end1, 0.0) - turned[1:2]
        rbuf[j, 0:2, :] = turned[2:4]
        return carry

    lax.fori_loop(0, blocks, backward, 0, unroll=4)

    since = (row >= lane).astype(F32)
    d_step = mm_exact(dcumbuf[...].reshape(flat), since)
    raw = dtrow[...].reshape(flat) + by_head(bias_ref)
    d_dt = rbuf[...].reshape(flat) / dt - d_step * rate
    d_raw = jnp.where(part < 2, d_dt * sigmoid(raw), 0.0)
    ddt_tx[...] = d_raw.astype(BF16).astype(F32).reshape(blocks, 8, 128)
    ga_part = jnp.sum((d_step * step).reshape(blocks, 8, 128), axis=0)

    def ddt_copy(peer, slot):
        return to(ddt_tx.at[peer], ddt_rx.at[slot], ddt_s.at[peer], ddt_r.at[slot], peer, seq)

    each(n_sp, lambda o: ddt_copy(ahead(o), me).start())
    some(early, n_sp, send_dz)

    def filters(i, carry):
        j = blocks - 1 - i
        at = rows(j)
        cums = cum_e[at, :]
        xs_hi, xs_lo = pair_at(xs_buf, at)
        ending = (xs_hi.astype(F32) + xs_lo.astype(F32)) * jnp.exp(cums[BLOCK - 1 : BLOCK] - cums)
        d_b = decay1[at, :] + mm3(split(ending), split(decay0[at, :]), 1, 1)
        dx_send[j] = unfiltered(x_slope[at, :], 0, wx).astype(BF16)
        bc_send[j, :, 0:STATE] = unfiltered(d_b * b_slope[at, :], 1, wb).astype(BF16)
        bc_send[j, :, STATE:] = unfiltered(c_slope[at, :], 2, wc).astype(BF16)
        return carry

    lax.fori_loop(0, blocks, filters, 0, unroll=2)
    partner = me + 1 - 2 * core
    pair_copies = lambda q: to(
        bc_send.at[2 * q + 1 - core], pair_rx.at[q], pair_s.at[q], pair_r.at[q], partner, seq
    )
    some(0, chips, lambda q: pair_copies(q).start())

    def send_dx(o):
        grad_copy(dx_send, dx_out, dx_s, dx_r, ahead(o), me).start()

    dx_early = min(DX_EARLY, n_sp - 1) + 1
    some(1, dx_early, send_dx)
    dx_own = pltpu.make_async_copy(dx_send.at[me], columns_of(dx_out, me), loc.at[7])
    dx_own.start()
    ddt_rx[me] = ddt_tx[me]
    each(n_sp, lambda o: ddt_copy(me, wrap(me + o, n_sp)).wait_recv())

    heads = 2 * n_sp
    source = lax.broadcasted_iota(jnp.int32, (heads, blocks * 8), 1)
    target = lax.broadcasted_iota(jnp.int32, (heads, blocks * 8), 0)
    pick = (source == (target // 2) * 8 + lax.rem(target, 2)).astype(BF16)
    own_ddt = mm(pick, ddt_rx[...].reshape(flat).astype(BF16)).astype(BF16)
    ddt_out[...] = own_ddt
    loads[4].wait()
    per_row = liv.shape[1] // 128

    ga_sum = jnp.broadcast_to(jnp.sum(ga_part, axis=1, keepdims=True), (8, 128))
    ga_tx[0] = ga_sum
    for c0 in range(0, per_row, 4):
        piece = mm(own_ddt, liv[:, c0 * 128 : (c0 + 4) * 128])
        for r in range(heads // 8):
            for c in range(4):
                t = r * per_row + c0 + c
                tile = piece[8 * r : 8 * r + 8, c * 128 : (c + 1) * 128]
                at = (t % w_tiles) * 8
                w_tx[t // w_tiles, at : at + 8, :] = tile.astype(BF16)

    def scatter_copy(k, slot):
        return to(w_tx.at[k], w_rx.at[slot], f_s.at[k], f_r.at[slot], me, k)

    each(n_dp, lambda o: scatter_copy(wrap(seq + hop(o, n_dp), n_dp), seq).start())

    n_edge = math.isqrt(n_dp)
    z_at = seq // n_edge
    y_at = lax.rem(seq, n_edge)

    def y_copy(k, slot):
        dst = ga_rx.at[0, slot]
        return to(ga_tx.at[0], dst, ga_s.at[0, k], ga_r.at[0, slot], me, z_at * n_edge + k)

    def z_copy(k, slot):
        dst = ga_rx.at[1, slot]
        return to(ga_tx.at[1], dst, ga_s.at[1, k], ga_r.at[1, slot], me, k * n_edge + y_at)

    each(n_edge, lambda o: y_copy(wrap(y_at + o, n_edge), y_at).start())

    def pair_add(q, c):
        pair_copies(q).wait_recv()
        mine = bc_send[2 * q + core].astype(F32)
        bc_sum[q] = (mine + pair_rx[q].astype(F32)).astype(BF16)
        return c

    lax.fori_loop(0, chips, pair_add, 0)

    w_rx[seq] = w_tx[seq]
    each(n_dp, lambda o: scatter_copy(seq, wrap(seq + o, n_dp)).wait_recv())
    sum2 = lax.fori_loop(
        1, n_dp, lambda k, t: t + w_rx[k].astype(F32), w_rx[0].astype(F32), unroll=3 if n_dp == 64 else 1
    )
    u_tx[...] = sum2

    def sp_copy(peer, slot):
        return to(u_tx, u_rx.at[slot], h_s.at[peer], h_r.at[slot], peer, seq)

    each(n_sp, lambda o: sp_copy(ahead(o), me).start())

    def bc_copy(q, slot):
        return to(bc_sum.at[q], bc_rx.at[slot], bc_s.at[q], bc_r.at[slot], 2 * q + core, seq)

    some(dx_early, n_sp, send_dx)
    each(chips, lambda o: bc_copy(wrap(chip + hop(o, chips), chips), chip).start())

    def summed(a):
        total = ga_rx[a, 0]
        for k in range(1, n_edge):
            total = total + ga_rx[a, k]
        return total

    ga_rx[0, y_at] = ga_tx[0]
    each(n_edge, lambda o: y_copy(y_at, wrap(y_at + o, n_edge)).wait_recv())
    ga_tx[1] = summed(0)
    each(n_edge, lambda o: z_copy(wrap(z_at + o, n_edge), z_at).start())
    ga_rx[1, z_at] = ga_tx[1]

    u_rx[me] = u_tx[...]
    each(n_sp, lambda o: sp_copy(me, wrap(me + o, n_sp)).wait_recv())
    sum3 = u_rx[0]
    for k in range(1, n_sp):
        sum3 = sum3 + u_rx[k]
    w_fin[seq] = sum3.astype(BF16)

    def gather_copy(k, slot):
        return to(w_fin.at[slot], w_fin.at[slot], k_s.at[k], k_r.at[slot], me, k)

    each(n_dp, lambda o: gather_copy(wrap(seq + hop(o, n_dp), n_dp), seq).start())

    each(n_edge, lambda o: z_copy(z_at, wrap(z_at + o, n_edge)).wait_recv())
    ga_out[...] = summed(1)

    bc_rx[chip] = bc_sum[chip]
    each(chips, lambda o: bc_copy(chip, wrap(chip + o, chips)).wait_recv())
    span = chips // GROUPS
    for g in range(GROUPS):
        total = bc_rx[g * span].astype(F32)
        for q in range(1, span):
            total = total + bc_rx[g * span + q].astype(F32)
        db_out[:, g * STATE : (g + 1) * STATE] = total[:, 0:STATE].astype(BF16)
        dc_out[:, g * STATE : (g + 1) * STATE] = total[:, STATE:].astype(BF16)

    def finish(o):
        peer = wrap(me + o, n_sp)
        cot_copy(peer, me).wait_send()
        ddt_copy(peer, me).wait_send()
        sp_copy(peer, me).wait_send()
        dz = grad_copy(dz_send, dz_out, dz_s, dz_r, peer, me)
        dz.wait_send()
        grad_copy(dz_send, dz_out, dz_s, dz_r, me, peer).wait_recv()
        grad_copy(dx_send, dx_out, dx_s, dx_r, peer, me).wait_send()
        grad_copy(dx_send, dx_out, dx_s, dx_r, me, peer).wait_recv()

    each(n_sp, finish)
    lax.fori_loop(0, chips, lambda q, c: (pair_copies(q).wait_send(), c)[1], 0)
    each(chips, lambda o: bc_copy(wrap(chip + o, chips), chip).wait_send())

    def finish_seq(o):
        peer = wrap(seq + o, n_dp)
        scatter_copy(peer, seq).wait_send()
        gather_copy(peer, seq).wait_send()
        gather_copy(seq, peer).wait_recv()

    each(n_dp, finish_seq)
    each(n_edge, lambda o: y_copy(wrap(y_at + o, n_edge), y_at).wait_send())
    each(n_edge, lambda o: z_copy(wrap(z_at + o, n_edge), z_at).wait_send())
    dz_own.wait()
    dx_own.wait()


def mixer(n_sp, n_dp, *args):
    n_edge = math.isqrt(n_dp)
    chips = n_sp // 2
    blocks = n_sp
    length = blocks * BLOCK
    width = n_sp * 128
    model = args[1].shape[1]
    heads = 2 * n_sp
    tiles = (heads // 8) * (model // 128)
    w_rows = 8 * tiles // n_dp
    any_space = pl.BlockSpec(memory_space=pl.ANY)
    vmem = pl.BlockSpec(memory_space=pltpu.VMEM)
    smem = pl.BlockSpec(memory_space=pltpu.SMEM)
    V = pltpu.VMEM
    seq_f = V((length, 128), F32)
    seq_b = V((length, 128), BF16)
    seq_d = V((length, 256), BF16)
    blk_b = V((blocks, BLOCK, 128), BF16)
    dma = lambda n: pltpu.SemaphoreType.DMA((n,))
    parts = pl.pallas_call(
        functools.partial(kernel, n_sp, n_dp),
        out_shape=(
            jax.ShapeDtypeStruct((BLOCK, width), BF16),
            jax.ShapeDtypeStruct((BLOCK, width), BF16),
            jax.ShapeDtypeStruct((BLOCK, GROUPS * STATE), BF16),
            jax.ShapeDtypeStruct((BLOCK, GROUPS * STATE), BF16),
            jax.ShapeDtypeStruct((heads, BLOCK), BF16),
            jax.ShapeDtypeStruct((8, 128), F32),
            jax.ShapeDtypeStruct((n_dp, w_rows, 128), BF16),
        ),
        in_specs=[any_space] * 6 + [vmem] * 5 + [smem] * 3,
        out_specs=(any_space, any_space) + (vmem,) * 5,
        scratch_shapes=[
            seq_b,
            seq_b,
            seq_b,
            seq_b,
            V((BLOCK, model), BF16),
            blk_b,
            V((blocks, 8, 128), F32),
            V((blocks, 8, 128), F32),
            V((blocks, 8, 128), F32),
            V((blocks, 8, 128), F32),
            seq_f,
            seq_d,
            seq_f,
            seq_d,
            seq_f,
            seq_f,
            seq_f,
            seq_f,
            V((length, 4 * BLOCK), BF16),
            seq_d,
            seq_f,
            seq_f,
            seq_f,
            seq_f,
            seq_f,
            seq_f,
            V((STATE, 128), F32),
            V((3, 8, 128), F32),
            blk_b,
            blk_b,
            V((blocks, BLOCK, 2 * STATE), BF16),
            V((chips, BLOCK, 2 * STATE), BF16),
            V((chips, BLOCK, 2 * STATE), BF16),
            V((chips, BLOCK, 2 * STATE), BF16),
            V((blocks, 8, 128), F32),
            V((blocks, 8, 128), F32),
            V((n_dp, w_rows, 128), BF16),
            V((n_dp, w_rows, 128), BF16),
            V((w_rows, 128), F32),
            V((n_sp, w_rows, 128), F32),
            V((2, 8, 128), F32),
            V((2, n_edge, 8, 128), F32),
            dma(8),
            dma(n_sp),
            dma(n_sp),
            dma(n_sp),
            dma(n_sp),
            dma(n_sp),
            dma(n_sp),
            dma(n_sp),
            dma(n_sp),
            dma(chips),
            dma(chips),
            dma(chips),
            dma(chips),
            dma(n_dp),
            dma(n_dp),
            dma(n_sp),
            dma(n_sp),
            dma(n_dp),
            dma(n_dp),
            pltpu.SemaphoreType.DMA((2, n_edge)),
            pltpu.SemaphoreType.DMA((2, n_edge)),
        ],
        compiler_params=pltpu.CompilerParams(
            collective_id=0, has_side_effects=True, vmem_limit_bytes=60000 * 1024
        ),
        name="mixer_backward",
    )(*args)
    return pl.pallas_call(
        finish_kernel,
        out_shape=tuple(jax.ShapeDtypeStruct(p.shape, p.dtype) for p in parts[:5])
        + (jax.ShapeDtypeStruct((2,), F32), jax.ShapeDtypeStruct((heads, model), F32)),
        in_specs=[vmem] * 7,
        out_specs=(vmem,) * 5 + (smem, vmem),
        name="finish",
    )(*parts)


def finish_kernel(dx, dz, db, dc, ddt, ga, w, dx_out, dz_out, db_out, dc_out, ddt_out, ga_out, gw_out):
    dx_out[...] = dx[...]
    dz_out[...] = dz[...]
    db_out[...] = db[...]
    dc_out[...] = dc[...]
    ddt_out[...] = ddt[...]
    ga_out[0] = ga[0, 0]
    ga_out[1] = ga[1, 0]
    per_row = gw_out.shape[1] // 128
    w_tiles = w.shape[1] // 8
    for t in range(w.shape[0] * w_tiles):
        r, c, at = t // per_row, t % per_row, 8 * (t % w_tiles)
        gw_out[8 * r : 8 * r + 8, c * 128 : (c + 1) * 128] = w[t // w_tiles, at : at + 8, :].astype(F32)


def shards(
    n_sp,
    n_dp,
    cotangent,
    layer_input,
    x_pre,
    z_pre,
    b_pre,
    c_pre,
    dt_raw,
    conv_x,
    conv_b,
    conv_c,
    dt_bias,
    a_log,
    d_skip,
    norm_w,
):
    dx, dz, db, dc, ddt, ga, gw = mixer(
        n_sp,
        n_dp,
        cotangent[0],
        layer_input[0],
        x_pre[0],
        z_pre[0],
        b_pre[0],
        c_pre[0],
        dt_raw[0].T,
        conv_x,
        conv_b,
        conv_c,
        norm_w[None],
        dt_bias,
        a_log,
        d_skip,
    )
    return (dx[None], dz[None], db[None], dc[None], ddt.T[None], ga, gw.T)


def solution(mesh):
    in_specs = (
        P("dp", "sp", None),
        P("dp", "sp", None),
        P("dp", None, "sp"),
        P("dp", None, "sp"),
        P("dp", None, None),
        P("dp", None, None),
        P("dp", None, "sp"),
        P(None, "sp"),
        P(),
        P(),
        P("sp"),
        P("sp"),
        P("sp"),
        P("sp"),
    )
    out_specs = (
        P("dp", "sp", None),
        P("dp", "sp", None),
        P("dp", "sp", None),
        P("dp", "sp", None),
        P("dp", "sp", None),
        P("sp"),
        P(),
    )
    return jax.shard_map(
        functools.partial(shards, mesh.shape["sp"], mesh.shape["dp"]),
        mesh=mesh,
        in_specs=in_specs,
        out_specs=out_specs,
        check_vma=False,
    )
```
